32 devices in a mesh: sp: 8 (over z, y), tp: 4 (over x, core).
Axes of the slice: x: 2, y: 2, z: 4, core: 2. Of those that a mesh axis runs over, the one named last changes fastest.
Arguments:
- arriving_hidden_state: bfloat16 [8192, 2048], P(('sp', 'tp')), may hold values from -6 to 6
- former_request_vectors: bfloat16 [8192, 1024], P('sp', 'tp'), may hold values from -6 to 6
- former_match_vectors: bfloat16 [8192, 1024], P('sp', 'tp'), may hold values from -6 to 6
- latter_request_vectors: bfloat16 [8192, 512], P('sp', 'tp'), may hold values from -6 to 6
- latter_match_vectors: bfloat16 [8192, 512], P('sp', 'tp'), may hold values from -6 to 6
- stored_vectors_both: bfloat16 [8192, 2, 1024], P('sp', None, 'tp'), may hold values from -6 to 6
- closing_valve_operands: bfloat16 [8192, 2, 1024], P('sp', None, 'tp'), may hold values from -6 to 6
- update_level_before_squash: bfloat16 [2, 8, 8192], P(None, 'tp', 'sp'), may hold values from -4 to -3
- fading_data_input: float32 [2, 8, 8192], P(None, 'tp', 'sp'), may hold values from -5.5 to 5.5
- sparse_fading_boost: float32 [2, 8, 8192], P(None, 'tp', 'sp'), may hold values from -2 to 0, as said below
- unitwise_fading_loglevel: float32 [2, 8], P(None, 'tp'), as said below
- fading_constant_term: float32 [2, 8], P(None, 'tp'), may hold values from -1 to 1
- unitwise_normalizer_coef: float32 [128], replicated, may hold values from 0.1 to 1.9
- emission_map_weights: bfloat16 [2048, 2048], replicated, may hold values from -0.125 to 0.125
- channel_normalizer_coef: float32 [2048], replicated, may hold values from 0.1 to 1.9
- switching_channel_map: bfloat16 [2048, 6144], P('sp', 'tp'), may hold values from -0.125 to 0.125
- broadening_channel_map: bfloat16 [2048, 6144], P('sp', 'tp'), may hold values from -0.125 to 0.125
- timewise_convolve_tapvalues: bfloat16 [3, 2, 6144], P(None, None, 'tp'), may hold values from -3.5 to 3.5
- narrowing_map_weights_in: bfloat16 [2048, 6144], P('sp', 'tp'), may hold values from -0.078125 to 0.078125
Outputs:
- mixed: bfloat16 [8192, 2048], P(('sp', 'tp'))
The draws below stay inside these ranges and needn't reach their ends.
Inputs may be any that keep to these rules, and one draw needn't show every extreme that they name: `unitwise_fading_loglevel`: each entry is the logarithm of a per-position rate between 0.2 / 8192 and 2 / 64. `sparse_fading_boost`: zero except at three or fewer positions of the sequence.
All inputs are finite; a program needn't handle non-finite values.
Results may differ from the reference program's by a relative error of at most 0.015.
Values may be sent and summed in bfloat16 or wider, within the bound.
A program may use at most 128 MiB of HBM per device.

```python
import jax
import jax.numpy as jnp
from jax import lax

MODEL_WIDTH = 2048
ATTN_UNITS = 8
DK_ONE = 128
DK_TWO = 64
VALUE_DIM = 128
FF = 6144
SPAN = 64
TAPS = 3
TOK_DEV = 1024
STEP_TOTAL = 8192
VW = 2048
N_TP = 4


def drawn_keys(key, column_count):
    direction_key, jitter_key = jax.random.split(key)
    directions = jax.random.normal(direction_key, (STEP_TOTAL // SPAN, column_count), jnp.float32)
    repeated = jnp.repeat(directions, SPAN, axis=0)
    jitter = jax.random.normal(jitter_key, (STEP_TOTAL, column_count), jnp.float32)
    jitter_scale = 0.2
    return jnp.clip(repeated + jitter_scale * jitter, -6.0, 6.0).astype(jnp.bfloat16)


def draw_former_match_vectors(key, part):
    return drawn_keys(jax.random.fold_in(key, 71), ATTN_UNITS * DK_ONE)


def draw_latter_match_vectors(key, part):
    return drawn_keys(jax.random.fold_in(key, 79), ATTN_UNITS * DK_TWO)


def draw_update_level_before_squash(key, part):
    drawn = jax.random.uniform(jax.random.fold_in(key, 53), (2, ATTN_UNITS, STEP_TOTAL), jnp.float32, -4.0, -3.0)
    return drawn.astype(jnp.bfloat16)


def draw_fading_data_input(key, part):
    noise_key, shift_key = jax.random.split(jax.random.fold_in(key, 11))
    noise_draw = jax.random.truncated_normal(noise_key, -4.0, 4.0, (2, ATTN_UNITS, STEP_TOTAL), jnp.float32)
    offsets = jax.random.uniform(shift_key, (2, ATTN_UNITS, STEP_TOTAL // TOK_DEV), jnp.float32, -1.5, 1.5)
    offset_rows = jnp.repeat(offsets, TOK_DEV, axis=2)
    return noise_draw + offset_rows


def draw_sparse_fading_boost(key, part):
    position_random_key, size_key = jax.random.split(jax.random.fold_in(key, 23))
    spike_positions = jax.random.randint(position_random_key, (3,), 0, STEP_TOTAL)
    kept_share = jax.random.uniform(size_key, (2, ATTN_UNITS, 3), jnp.float32, 0.55, 0.8)
    position_hits = (jnp.arange(STEP_TOTAL)[None, :] == spike_positions[:, None]).astype(jnp.float32)
    return jnp.einsum('ghb,bs->ghs', jnp.log(kept_share), position_hits)


def draw_unitwise_fading_loglevel(key, part):
    pick_key, fast_key, slow_key = jax.random.split(jax.random.fold_in(key, 37), 3)
    fast_share = 0.5
    fast_mask = jax.random.uniform(pick_key, (2, ATTN_UNITS), jnp.float32) < fast_share
    fast_rate = jax.random.uniform(fast_key, (2, ATTN_UNITS), jnp.float32, 1.0, 2.0) / SPAN
    slow_rate = jax.random.uniform(slow_key, (2, ATTN_UNITS), jnp.float32, 0.2, 0.4) / STEP_TOTAL
    return jnp.log(jnp.where(fast_mask, fast_rate, slow_rate))


def level_of(key, dims, cuts, smallest, high):
    loudness, own = 1.0, jax.random.fold_in(key, 6)
    for axis_at, shards_of in cuts:
        heights = jnp.exp(jax.random.uniform(jax.random.fold_in(own, axis_at), (shards_of,), jnp.float32, smallest / len(cuts), high / len(cuts)))
        loudness = loudness * jnp.repeat(heights, dims[axis_at] // shards_of).reshape([-1 if axis == axis_at else 1 for axis in range(len(dims))])
    return loudness


def gaussian(rng, shape, scale, most, shards=(), kind=jnp.bfloat16):
    entries = jax.random.normal(rng, shape, jnp.float32) * scale
    if len(shards) > 0:
        entries = level_of(rng, shape, shards, -0.22, 0.18) * entries
    return jnp.clip(entries, min=-most, max=most).astype(kind)


def setup_inputs(seed: int = 0) -> dict:
    streams_of = jax.random.split(jax.random.key(seed), 20)
    return {
        "arriving_hidden_state": gaussian(streams_of[0], (STEP_TOTAL, MODEL_WIDTH), 1.0, 6.0, ((0, 32),)),
        "former_request_vectors": gaussian(streams_of[1], (STEP_TOTAL, ATTN_UNITS * DK_ONE), 1.0, 6.0, ((0, 8), (1, 4))),
        "former_match_vectors": draw_former_match_vectors(jax.random.fold_in(streams_of[19], 71), 0),
        "latter_request_vectors": gaussian(streams_of[3], (STEP_TOTAL, ATTN_UNITS * DK_TWO), 1.0, 6.0, ((0, 8), (1, 4))),
        "latter_match_vectors": draw_latter_match_vectors(jax.random.fold_in(streams_of[19], 71), 0),
        "stored_vectors_both": gaussian(streams_of[5], (STEP_TOTAL, 2, ATTN_UNITS * VALUE_DIM), 1.0, 6.0, ((0, 8), (2, 4))),
        "closing_valve_operands": gaussian(streams_of[6], (STEP_TOTAL, 2, ATTN_UNITS * VALUE_DIM), 1.0, 6.0, ((0, 8), (2, 4))),
        "update_level_before_squash": draw_update_level_before_squash(jax.random.fold_in(streams_of[19], 71), 0),
        "fading_data_input": draw_fading_data_input(jax.random.fold_in(streams_of[19], 71), 0),
        "sparse_fading_boost": draw_sparse_fading_boost(jax.random.fold_in(streams_of[19], 71), 0),
        "unitwise_fading_loglevel": draw_unitwise_fading_loglevel(jax.random.fold_in(streams_of[19], 71), 0),
        "fading_constant_term": jnp.clip(jax.random.uniform(streams_of[11], (2, ATTN_UNITS), jnp.float32, -1.0, 1.0) * level_of(streams_of[11], (2, ATTN_UNITS), ((1, 4),), -0.4, 0.0), -1.0, 1.0),
        "unitwise_normalizer_coef": jnp.clip(1.0 + 0.18 * jax.random.normal(streams_of[12], (VALUE_DIM,), jnp.float32), 0.1, 1.9),
        "emission_map_weights": gaussian(streams_of[13], (VW, MODEL_WIDTH), VW ** -0.5, 0.125),
        "channel_normalizer_coef": jnp.clip(1.0 + 0.18 * jax.random.normal(streams_of[14], (MODEL_WIDTH,), jnp.float32), 0.1, 1.9),
        "switching_channel_map": gaussian(streams_of[15], (MODEL_WIDTH, FF), MODEL_WIDTH ** -0.5, 0.125, ((0, 8), (1, 4))),
        "broadening_channel_map": gaussian(streams_of[16], (MODEL_WIDTH, FF), MODEL_WIDTH ** -0.5, 0.125, ((0, 8), (1, 4))),
        "timewise_convolve_tapvalues": gaussian(streams_of[17], (TAPS, 2, FF), TAPS ** -0.5, 3.5, ((2, 4),)),
        "narrowing_map_weights_in": gaussian(streams_of[18], (MODEL_WIDTH, FF), FF ** -0.5, 0.078125, ((0, 8), (1, 4))),
    }


EPSILON = 1e-06
PRECISE = lax.Precision.HIGHEST

def unit_rows(matrix):
    return matrix * lax.rsqrt(lax.optimization_barrier(jnp.sum(matrix * matrix, axis=-1, keepdims=True)) + EPSILON)

def heads_first(matrix, head_count):
    row_count = matrix.shape[0]
    return matrix.reshape(row_count, head_count, -1).astype(jnp.float32).transpose(1, 0, 2)

def block_terms(queries, key_rows, value_rows, beta_rate, gate_logarithms):
    head_count, length, key_size = queries.shape
    num_blocks = length // SPAN
    queries = queries.reshape(head_count, num_blocks, SPAN, -1)
    key_rows = key_rows.reshape(head_count, num_blocks, SPAN, -1)
    value_rows = value_rows.reshape(head_count, num_blocks, SPAN, -1)
    beta_rate = beta_rate.reshape(head_count, num_blocks, SPAN)
    cum_gates = jnp.cumsum(gate_logarithms.reshape(head_count, num_blocks, SPAN), axis=-1)
    row_pos = lax.broadcasted_iota(jnp.int32, (SPAN, SPAN), 0)
    col_pos = lax.broadcasted_iota(jnp.int32, (SPAN, SPAN), 1)
    causal = row_pos >= col_pos
    strict = row_pos > col_pos
    decay = jnp.exp(jnp.where(causal, cum_gates[..., :, None] - cum_gates[..., None, :], -jnp.inf))
    key_beta = key_rows * beta_rate[..., None]
    lower = jnp.where(strict, jnp.einsum('hncd,hnsd->hncs', key_beta, key_rows, precision=PRECISE) * decay, 0.0)
    right_side = jnp.concatenate([value_rows * beta_rate[..., None], key_beta * jnp.exp(cum_gates)[..., None]], axis=-1)
    unit_mat = jnp.eye(SPAN, dtype=lower.dtype)
    solved = lax.linalg.triangular_solve(lower + unit_mat, right_side, left_side=True, lower=True, unit_diagonal=True)
    value_size = value_rows.shape[-1]
    u_values = solved[..., :value_size]
    w_keys = solved[..., value_size:]
    intra = jnp.einsum('hncd,hnsd->hncs', queries, key_rows, precision=PRECISE) * decay
    key_decayed = key_rows * jnp.exp(cum_gates[..., -1:] - cum_gates)[..., None]
    return (queries, u_values, w_keys, intra, key_decayed, cum_gates)

def run_blocks(increment_list, initial_memory):

    def advance(state_mat, inputs):
        query_blk, u_blk, w_blk, intra_blk, kdec_blk, cum_blk = inputs
        fresh = u_blk - jnp.einsum('hcd,hde->hce', w_blk, state_mat, precision=PRECISE)
        output = jnp.einsum('hcd,hde->hce', query_blk * jnp.exp(cum_blk)[..., None], state_mat, precision=PRECISE)
        output = output + jnp.einsum('hcs,hse->hce', intra_blk, fresh, precision=PRECISE)
        state_mat = state_mat * jnp.exp(cum_blk[:, -1])[:, None, None]
        state_mat = state_mat + jnp.einsum('hcd,hce->hde', kdec_blk, fresh, precision=PRECISE)
        return (state_mat, output)
    moved = tuple((jnp.moveaxis(member, 1, 0) for member in increment_list))
    _, outputs = lax.scan(advance, initial_memory, moved)
    head_count = outputs.shape[1]
    return jnp.moveaxis(outputs, 0, 1).reshape(head_count, -1, outputs.shape[-1])

def team_parts(asker_weights, lookup_weights, value_matrix, correction_draw, decay_draw, spike_draw, decay_logarithm, bias_vector):
    head_count = decay_logarithm.shape[0]
    queries = heads_first(asker_weights, head_count)
    key_size = queries.shape[-1]
    queries = unit_rows(queries) * key_size ** (-0.5)
    key_rows = unit_rows(heads_first(lookup_weights, head_count))
    value_rows = heads_first(value_matrix, head_count)
    beta_rate = jax.nn.sigmoid(correction_draw.astype(jnp.float32))
    gate_logarithms = -jnp.exp(decay_logarithm)[:, None] * jax.nn.softplus(decay_draw + bias_vector[:, None]) + spike_draw
    return block_terms(queries, key_rows, value_rows, beta_rate, gate_logarithms)

def completed_attn_units(increment_list, initial_memory, gate_cols, unitwise_normalizer_coef):
    outputs = run_blocks(increment_list, initial_memory)
    head_count = outputs.shape[0]
    gates_in = heads_first(gate_cols, head_count)
    scaled = outputs * lax.rsqrt(lax.optimization_barrier(jnp.mean(outputs * outputs, axis=-1, keepdims=True)) + EPSILON) * unitwise_normalizer_coef
    scaled = scaled * jax.nn.silu(gates_in)
    return scaled.transpose(1, 0, 2).reshape(outputs.shape[1], -1).astype(jnp.bfloat16)

def causal_taps(low_rows, taps_col):
    padded = jnp.concatenate([jnp.zeros((TAPS - 1, low_rows.shape[1]), low_rows.dtype), low_rows], axis=0)
    length = low_rows.shape[0]
    total = taps_col[0] * padded[0:length]
    for tap_index in range(1, TAPS):
        total = total + taps_col[tap_index] * padded[tap_index:tap_index + length]
    return total

def reference(arriving_hidden_state, former_request_vectors, former_match_vectors, latter_request_vectors, latter_match_vectors, stored_vectors_both, closing_valve_operands, update_level_before_squash, fading_data_input, sparse_fading_boost, unitwise_fading_loglevel, fading_constant_term, unitwise_normalizer_coef, emission_map_weights, channel_normalizer_coef, switching_channel_map, broadening_channel_map, timewise_convolve_tapvalues, narrowing_map_weights_in):
    combined_attn_units = []
    pairs = ((former_request_vectors, former_match_vectors), (latter_request_vectors, latter_match_vectors))
    for cohort_ordinal in range(2):
        asker_weights, lookup_weights = pairs[cohort_ordinal]
        increment_list = team_parts(asker_weights, lookup_weights, stored_vectors_both[:, cohort_ordinal], update_level_before_squash[cohort_ordinal], fading_data_input[cohort_ordinal], sparse_fading_boost[cohort_ordinal], unitwise_fading_loglevel[cohort_ordinal], fading_constant_term[cohort_ordinal])
        key_size = increment_list[0].shape[-1]
        head_count = unitwise_fading_loglevel.shape[1]
        initial_memory = jnp.zeros((head_count, key_size, stored_vectors_both.shape[-1] // head_count), jnp.float32)
        combined_attn_units.append(completed_attn_units(increment_list, initial_memory, closing_valve_operands[:, cohort_ordinal], unitwise_normalizer_coef))
    linear_attend = jnp.stack(combined_attn_units, axis=1)
    token_slices = linear_attend.shape[0]
    skip_stream = arriving_hidden_state.astype(jnp.float32) + jnp.dot(linear_attend.reshape(token_slices, -1).astype(jnp.float32), emission_map_weights.astype(jnp.float32), preferred_element_type=jnp.float32)
    normed = (skip_stream * lax.rsqrt(lax.optimization_barrier(jnp.mean(skip_stream * skip_stream, axis=-1, keepdims=True)) + EPSILON) * channel_normalizer_coef).astype(jnp.bfloat16)
    gate_low = jnp.dot(normed.astype(jnp.float32), switching_channel_map.astype(jnp.float32), preferred_element_type=jnp.float32).astype(jnp.bfloat16)
    up_low = jnp.dot(normed.astype(jnp.float32), broadening_channel_map.astype(jnp.float32), preferred_element_type=jnp.float32).astype(jnp.bfloat16)
    taps = timewise_convolve_tapvalues.astype(jnp.float32)
    gate_conv = causal_taps(gate_low, taps[:, 0])
    up_conv = causal_taps(up_low, taps[:, 1])
    hidden = (jax.nn.silu(gate_conv) * up_conv).astype(jnp.bfloat16)
    shard_width = hidden.shape[1] // N_TP
    down_sum = jnp.zeros(skip_stream.shape, jnp.float32)
    for shard_index in range(N_TP):
        lower_col = shard_index * shard_width
        partial_value = lax.dot_general(hidden[:, lower_col:lower_col + shard_width].astype(jnp.float32), narrowing_map_weights_in[:, lower_col:lower_col + shard_width].astype(jnp.float32), (((1,), (1,)), ((), ())), preferred_element_type=jnp.float32)
        down_sum = down_sum + lax.optimization_barrier(partial_value.astype(jnp.bfloat16)).astype(jnp.float32)
    return (skip_stream + down_sum).astype(jnp.bfloat16)
```

```python
import functools

import jax
import jax.numpy as jnp
from jax import lax
from jax.experimental import pallas as pl
from jax.experimental.pallas import tpu as pltpu
from jax.sharding import PartitionSpec as P

TAPS = 3
CHUNK = 128
BASE = 16
LANES = 128

EPSILON = 1e-06
F32 = jnp.float32
BF16 = jnp.bfloat16


def from_behind(value, axis, steps):
    count = lax.axis_size(axis)
    leading, last = (max(0, -steps), min(count, count - steps))
    return lax.ppermute(value, axis, [(source, source + steps) for source in range(leading, last)])


def mm(a, b):
    return jnp.dot(a.astype(BF16), b.astype(BF16), preferred_element_type=F32)


def mm_nt(a, b):
    return lax.dot_general(
        a.astype(BF16), b.astype(BF16), (((1,), (1,)), ((), ())), preferred_element_type=F32
    )


def mm_tn(a, b):
    return mm(a.T, b)


def local_kernel(q1_ref, k1_ref, q2_ref, k2_ref, v_ref, gb_ref, g_ref, h_ref, last_ref, run_ref):
    step = pl.program_id(0)
    count = v_ref.shape[1] // LANES // 2
    pair = LANES // (LANES // 2)
    rows = lax.broadcasted_iota(jnp.int32, (CHUNK, CHUNK), 0)
    cols = lax.broadcasted_iota(jnp.int32, (CHUNK, CHUNK), 1)
    eye = (rows == cols).astype(F32)
    causal = rows >= cols
    strict = rows > cols
    lane = lax.broadcasted_iota(jnp.int32, (1, LANES), 1)

    @pl.when(step == 0)
    def _():
        for unit in range(run_ref.shape[0]):
            run_ref[unit, :, :LANES] = jnp.zeros((LANES, LANES), F32)
            run_ref[unit, :, LANES:] = eye

    gb = gb_ref[...]
    cum = gb
    lanes8 = lax.broadcasted_iota(jnp.int32, gb.shape, 1)
    shift = 1
    while shift < CHUNK:
        cum = cum + jnp.where(lanes8 >= shift, pltpu.roll(cum, shift, 1), 0.0)
        shift *= 2
    gbt = gb.T
    cumt = cum.T

    pend = None
    for head in range(2 * count):
        group, at = head // count, head % count
        if group == 0:
            q = q1_ref[:, at * LANES : (at + 1) * LANES].astype(F32)
            k = k1_ref[:, at * LANES : (at + 1) * LANES].astype(F32)
            key_size = LANES
            own = None
        else:
            key_size = LANES // 2
            own = (lane // key_size) == at % pair
            first = (at // pair) * LANES
            q = jnp.where(own, q2_ref[:, first : first + LANES].astype(F32), 0.0)
            k = jnp.where(own, k2_ref[:, first : first + LANES].astype(F32), 0.0)
        q = q * (lax.rsqrt(jnp.sum(q * q, axis=-1, keepdims=True) + EPSILON) * key_size ** (-0.5))
        k = k * lax.rsqrt(jnp.sum(k * k, axis=-1, keepdims=True) + EPSILON)
        v = v_ref[:, head * LANES : (head + 1) * LANES].astype(F32)
        beta = gbt[:, 2 * count + head : 2 * count + head + 1]
        cum_col = cumt[:, head : head + 1]
        cum_row = cum[head : head + 1, :]
        total = cum[head : head + 1, CHUNK - 1 : CHUNK]
        decay = jnp.exp(jnp.where(causal, cum_col - cum_row, -1e30))
        grown = jnp.exp(cum_col)
        kbeta = k * beta
        kbf = k.astype(BF16)
        low = jnp.where(strict, mm_nt(kbeta, kbf) * decay, 0.0)
        intra = mm_nt(q, kbf) * decay
        base = jnp.where((rows // BASE) == (cols // BASE), low, 0.0)
        power = -base
        inv = eye + power
        size = 2
        while size < BASE:
            power = mm(power, power)
            inv = inv + mm(inv, power)
            size *= 2
        block = BASE
        while block < CHUNK:
            off = jnp.where(
                ((rows // (2 * block)) == (cols // (2 * block)))
                & ((rows // block) != (cols // block)),
                low,
                0.0,
            )
            inv = inv - mm(mm(inv, off), inv)
            block *= 2
        right = jnp.concatenate([v * beta, kbeta * grown], axis=-1)
        solved = mm(inv, right)
        kdec = k * jnp.exp(total - cum_col)
        both = mm_tn(kdec, solved)
        inner = mm(intra, solved)
        unit_diag = eye if own is None else jnp.where(own, eye, 0.0)
        cmap = jnp.exp(total) * unit_diag - both[:, LANES:]
        cadd = both[:, :LANES]
        pmat = q * grown - inner[:, LANES:]
        unit = head if group == 0 else count + at // pair
        run = run_ref[unit]
        seen = mm(pmat, run)
        h_ref[:, head * LANES : (head + 1) * LANES] = seen[:, :LANES] + inner[:, :LANES]
        g_ref[:, head * LANES : (head + 1) * LANES] = seen[:, LANES:].astype(g_ref.dtype)
        if pend is not None:
            cmap = cmap + pend[0]
            cadd = cadd + pend[1]
            pend = None
        if group == 1 and at % pair != pair - 1 and at != count - 1:
            pend = (cmap, cadd)
            continue
        nxt = mm(cmap, run)
        run_ref[unit, :, :LANES] = nxt[:, :LANES] + cadd
        run_ref[unit, :, LANES:] = nxt[:, LANES:]

    @pl.when(step == pl.num_programs(0) - 1)
    def _():
        last_ref[...] = run_ref[...].astype(last_ref.dtype)


def local_terms(q1, k1, q2, k2, values, gates_beta):
    length = q1.shape[0]
    wide = values.shape[1]
    steps = length // CHUNK
    units = q1.shape[1] // LANES + q2.shape[1] // LANES
    return pl.pallas_call(
        local_kernel,
        grid=(steps,),
        in_specs=[
            pl.BlockSpec((CHUNK, q1.shape[1]), lambda i: (i, 0)),
            pl.BlockSpec((CHUNK, k1.shape[1]), lambda i: (i, 0)),
            pl.BlockSpec((CHUNK, q2.shape[1]), lambda i: (i, 0)),
            pl.BlockSpec((CHUNK, k2.shape[1]), lambda i: (i, 0)),
            pl.BlockSpec((CHUNK, wide), lambda i: (i, 0)),
            pl.BlockSpec((gates_beta.shape[0], CHUNK), lambda i: (0, i)),
        ],
        out_specs=[
            pl.BlockSpec((CHUNK, wide), lambda i: (i, 0)),
            pl.BlockSpec((CHUNK, wide), lambda i: (i, 0)),
            pl.BlockSpec((units, LANES, 2 * LANES), lambda i: (0, 0, 0)),
        ],
        out_shape=[
            jax.ShapeDtypeStruct((length, wide), BF16),
            jax.ShapeDtypeStruct((length, wide), F32),
            jax.ShapeDtypeStruct((units, LANES, 2 * LANES), BF16),
        ],
        scratch_shapes=[pltpu.VMEM((units, LANES, 2 * LANES), F32)],
        cost_estimate=pl.CostEstimate(
            flops=steps * 4 * 60 * CHUNK**3, bytes_accessed=length * wide * 10, transcendentals=0
        ),
    )(q1, k1, q2, k2, values, gates_beta)


def finish_kernel(place_ref, all_ref, g_ref, h_ref, gate_ref, coef_ref, out_ref, state_ref):
    @pl.when(pl.program_id(0) == 0)
    def _():
        state_ref[...] = jnp.zeros_like(state_ref)

        def turn(i, carry):
            for unit in range(all_ref.shape[1]):
                block = all_ref[i, unit]
                state_ref[unit] = (
                    mm(block[:, LANES:], state_ref[unit]) + block[:, :LANES].astype(F32)
                )
            return carry

        lax.fori_loop(0, place_ref[0], turn, 0)

    coef = coef_ref[...]
    count = out_ref.shape[1] // LANES // 2
    for head in range(2 * count):
        unit = head if head < count else count + (head - count) // 2
        at = pl.ds(head * LANES, LANES)
        out = mm(g_ref[:, at], state_ref[unit]) + h_ref[:, at]
        gate = gate_ref[:, at].astype(F32)
        scaled = out * lax.rsqrt(jnp.mean(out * out, axis=-1, keepdims=True) + EPSILON) * coef
        out_ref[:, at] = (scaled * (gate / (1.0 + jnp.exp(-gate)))).astype(out_ref.dtype)


def finish_heads(place, everyone, g, h, gates, coef):
    length, wide = g.shape
    tile = min(256, length)
    return pl.pallas_call(
        finish_kernel,
        grid_spec=pltpu.PrefetchScalarGridSpec(
            num_scalar_prefetch=1,
            grid=(length // tile,),
            in_specs=[
                pl.BlockSpec(everyone.shape, lambda i, p: (0, 0, 0, 0)),
                pl.BlockSpec((tile, wide), lambda i, p: (i, 0)),
                pl.BlockSpec((tile, wide), lambda i, p: (i, 0)),
                pl.BlockSpec((tile, wide), lambda i, p: (i, 0)),
                pl.BlockSpec((1, LANES), lambda i, p: (0, 0)),
            ],
            out_specs=pl.BlockSpec((tile, wide), lambda i, p: (i, 0)),
            scratch_shapes=[pltpu.VMEM((everyone.shape[1], LANES, LANES), F32)],
        ),
        out_shape=jax.ShapeDtypeStruct((length, wide), BF16),
        cost_estimate=pl.CostEstimate(
            flops=2 * length * wide * LANES * 8, bytes_accessed=length * wide * 10, transcendentals=0
        ),
    )(place, everyone, g, h, gates, coef)


def causal_taps(edge_rows, low_rows, taps_col):
    padded = jnp.concatenate([edge_rows, low_rows], axis=0)
    length = low_rows.shape[0]
    total = taps_col[0] * padded[0:length]
    for tap_index in range(1, TAPS):
        total = total + taps_col[tap_index] * padded[tap_index : tap_index + length]
    return total


def per_device(
    arriving_hidden_state,
    former_request_vectors,
    former_match_vectors,
    latter_request_vectors,
    latter_match_vectors,
    stored_vectors_both,
    closing_valve_operands,
    update_level_before_squash,
    fading_data_input,
    sparse_fading_boost,
    unitwise_fading_loglevel,
    fading_constant_term,
    unitwise_normalizer_coef,
    emission_map_weights,
    channel_normalizer_coef,
    switching_channel_map,
    broadening_channel_map,
    timewise_convolve_tapvalues,
    narrowing_map_weights_in,
):
    whole_gate, whole_up, whole_down = (
        lax.all_gather(switching_channel_map, "sp", axis=0, tiled=True),
        lax.all_gather(broadening_channel_map, "sp", axis=0, tiled=True),
        lax.all_gather(narrowing_map_weights_in, "sp", axis=0, tiled=True),
    )
    length = former_request_vectors.shape[0]
    level = (
        -jnp.exp(unitwise_fading_loglevel)[..., None]
        * jax.nn.softplus(fading_data_input + fading_constant_term[..., None])
        + sparse_fading_boost
    )
    beta_rate = jax.nn.sigmoid(update_level_before_squash.astype(jnp.float32))
    gates_beta = jnp.concatenate([level, beta_rate], axis=0).reshape(-1, length)
    gates_beta = jnp.pad(gates_beta, ((0, -gates_beta.shape[0] % 8), (0, 0)))
    spare = -latter_request_vectors.shape[1] % LANES
    g_part, h_part, summary = local_terms(
        former_request_vectors,
        former_match_vectors,
        jnp.pad(latter_request_vectors, ((0, 0), (0, spare))),
        jnp.pad(latter_match_vectors, ((0, 0), (0, spare))),
        stored_vectors_both.reshape(length, -1),
        gates_beta,
    )
    everyone = lax.all_gather(summary, "sp")
    place = lax.axis_index("sp").astype(jnp.int32).reshape(1)
    attended = finish_heads(
        place,
        everyone,
        g_part,
        h_part,
        closing_valve_operands.reshape(length, -1),
        unitwise_normalizer_coef.reshape(1, -1),
    )
    linear_attend = attended.reshape(length, 2, -1)
    arrived = lax.all_to_all(linear_attend, "tp", split_axis=0, concat_axis=2, tiled=True)
    row_count = arrived.shape[0]
    skip_stream = arriving_hidden_state.astype(jnp.float32) + jnp.dot(
        arrived.reshape(row_count, -1), emission_map_weights, preferred_element_type=jnp.float32
    )
    normed = (
        skip_stream
        * lax.rsqrt(jnp.mean(skip_stream * skip_stream, axis=-1, keepdims=True) + EPSILON)
        * channel_normalizer_coef
    ).astype(jnp.bfloat16)
    features = lax.all_gather(normed, "tp", axis=0, tiled=True)
    gate_full = jnp.dot(features, whole_gate, preferred_element_type=jnp.float32)
    up_full = jnp.dot(features, whole_up, preferred_element_type=jnp.float32)
    gate_low = gate_full.astype(jnp.bfloat16)
    up_low = up_full.astype(jnp.bfloat16)
    edge_gate, edge_up = from_behind((gate_low[-(TAPS - 1) :], up_low[-(TAPS - 1) :]), "sp", 1)
    taps = timewise_convolve_tapvalues.astype(jnp.float32)
    gate_conv = causal_taps(edge_gate, gate_low, taps[:, 0])
    up_conv = causal_taps(edge_up, up_low, taps[:, 1])
    hidden = (jax.nn.silu(gate_conv) * up_conv).astype(jnp.bfloat16)
    down_sum = lax.psum_scatter(
        lax.dot_general(
            hidden, whole_down, (((1,), (1,)), ((), ())), preferred_element_type=jnp.float32
        ).astype(jnp.bfloat16),
        "tp",
        scatter_dimension=0,
        tiled=True,
    ).astype(jnp.float32)
    return (skip_stream + down_sum).astype(jnp.bfloat16)


def solution(mesh):
    placed = (
        P(("sp", "tp"), None),
        P("sp", "tp"),
        P("sp", "tp"),
        P("sp", "tp"),
        P("sp", "tp"),
        P("sp", None, "tp"),
        P("sp", None, "tp"),
        P(None, "tp", "sp"),
        P(None, "tp", "sp"),
        P(None, "tp", "sp"),
        P(None, "tp"),
        P(None, "tp"),
        P(),
        P(),
        P(),
        P("sp", "tp"),
        P("sp", "tp"),
        P(None, None, "tp"),
        P("sp", "tp"),
    )
    return jax.shard_map(
        per_device, mesh=mesh, in_specs=placed, out_specs=P(("sp", "tp"), None), check_vma=False
    )
```

```python
import functools

import jax
import jax.numpy as jnp
from jax import lax
from jax.experimental import pallas as pl
from jax.experimental.pallas import tpu as pltpu
from jax.sharding import PartitionSpec as P

TAPS = 3
CHUNK = 128
BASE = 16
LANES = 128

EPSILON = 1e-06
F32 = jnp.float32
BF16 = jnp.bfloat16


def from_behind(value, axis, steps):
    count = lax.axis_size(axis)
    leading, last = (max(0, -steps), min(count, count - steps))
    return lax.ppermute(value, axis, [(source, source + steps) for source in range(leading, last)])


def mm(a, b):
    return jnp.dot(a.astype(BF16), b.astype(BF16), preferred_element_type=F32)


def mm_nt(a, b):
    return lax.dot_general(
        a.astype(BF16), b.astype(BF16), (((1,), (1,)), ((), ())), preferred_element_type=F32
    )


def mm_tn(a, b):
    return mm(a.T, b)


def local_kernel(
    q1_ref, k1_ref, q2_ref, k2_ref, v_ref, gb_ref, from_ref, *rest
):
    g_ref, h_ref, last_ref, sum_ref, run_ref = rest[-5:]
    step = pl.program_id(0)
    count = v_ref.shape[1] // LANES // 2
    pair = 2
    rows = lax.broadcasted_iota(jnp.int32, (CHUNK, CHUNK), 0)
    cols = lax.broadcasted_iota(jnp.int32, (CHUNK, CHUNK), 1)
    eye = (rows == cols).astype(F32)
    causal = rows >= cols
    strict = rows > cols
    lane = lax.broadcasted_iota(jnp.int32, (1, LANES), 1)

    @pl.when(step == 0)
    def _():
        run_ref[...] = from_ref[...]

    gb = gb_ref[...]
    cum = gb
    lanes8 = lax.broadcasted_iota(jnp.int32, gb.shape, 1)
    shift = 1
    while shift < CHUNK:
        cum = cum + jnp.where(lanes8 >= shift, pltpu.roll(cum, shift, 1), 0.0)
        shift *= 2
    gbt = gb.T
    cumt = cum.T

    pend = None
    for head in range(2 * count):
        group, at = head // count, head % count
        if group == 0:
            q = q1_ref[:, at * LANES : (at + 1) * LANES].astype(F32)
            k = k1_ref[:, at * LANES : (at + 1) * LANES].astype(F32)
            key_size = LANES
            own = None
        else:
            key_size = LANES // 2
            own = (lane // key_size) == at % pair
            first = (at // pair) * LANES
            q = jnp.where(own, q2_ref[:, first : first + LANES].astype(F32), 0.0)
            k = jnp.where(own, k2_ref[:, first : first + LANES].astype(F32), 0.0)
        q = q * (lax.rsqrt(jnp.sum(q * q, axis=-1, keepdims=True) + EPSILON) * key_size ** (-0.5))
        k = k * lax.rsqrt(jnp.sum(k * k, axis=-1, keepdims=True) + EPSILON)
        v = v_ref[:, head * LANES : (head + 1) * LANES].astype(F32)
        beta = gbt[:, 2 * count + head : 2 * count + head + 1]
        cum_col = cumt[:, head : head + 1]
        cum_row = cum[head : head + 1, :]
        total = cum[head : head + 1, CHUNK - 1 : CHUNK]
        decay = jnp.exp(jnp.where(causal, cum_col - cum_row, -1e30))
        grown = jnp.exp(cum_col)
        kbeta = k * beta
        kbf = k.astype(BF16)
        low = jnp.where(strict, mm_nt(kbeta, kbf) * decay, 0.0)
        intra = mm_nt(q, kbf) * decay
        base = jnp.where((rows // BASE) == (cols // BASE), low, 0.0)
        power = -base
        inv = eye + power
        size = 2
        while size < BASE:
            power = mm(power, power)
            inv = inv + mm(inv, power)
            size *= 2
        block = BASE
        while block < CHUNK:
            off = jnp.where(
                ((rows // (2 * block)) == (cols // (2 * block)))
                & ((rows // block) != (cols // block)),
                low,
                0.0,
            )
            inv = inv - mm(mm(inv, off), inv)
            block *= 2
        right = jnp.concatenate([v * beta, kbeta * grown], axis=-1)
        solved = mm(inv, right)
        kdec = k * jnp.exp(total - cum_col)
        both = mm_tn(kdec, solved)
        inner = mm(intra, solved)
        unit_diag = eye if own is None else jnp.where(own, eye, 0.0)
        cmap = jnp.exp(total) * unit_diag - both[:, LANES:]
        cadd = both[:, :LANES]
        pmat = q * grown - inner[:, LANES:]
        unit = head if group == 0 else count + at // pair
        run = run_ref[unit]
        seen = mm(pmat, run)
        h_ref[:, head * LANES : (head + 1) * LANES] = seen[:, :LANES] + inner[:, :LANES]
        g_ref[:, head * LANES : (head + 1) * LANES] = seen[:, LANES:].astype(g_ref.dtype)
        if pend is not None:
            cmap = cmap + pend[0]
            cadd = cadd + pend[1]
            pend = None
        if group == 1 and at % pair != pair - 1 and at != count - 1:
            pend = (cmap, cadd)
            continue
        nxt = mm(cmap, run)
        run_ref[unit, :, :LANES] = nxt[:, :LANES] + cadd
        run_ref[unit, :, LANES:] = nxt[:, LANES:]

    @pl.when(step == pl.num_programs(0) - 1)
    def _():
        last_ref[...] = run_ref[...]
        sum_ref[...] = run_ref[...].astype(sum_ref.dtype)


def local_terms(q1, k1, q2, k2, values, gates_beta, running, part, parts, earlier):
    length = q1.shape[0]
    wide = values.shape[1]
    steps = length // CHUNK // parts
    base = part * steps
    units = running.shape[0]
    whole = pl.BlockSpec((units, LANES, 2 * LANES), lambda i: (0, 0, 0))
    return pl.pallas_call(
        local_kernel,
        grid=(steps,),
        in_specs=[
            pl.BlockSpec((CHUNK, q1.shape[1]), lambda i: (i + base, 0)),
            pl.BlockSpec((CHUNK, k1.shape[1]), lambda i: (i + base, 0)),
            pl.BlockSpec((CHUNK, q2.shape[1]), lambda i: (i + base, 0)),
            pl.BlockSpec((CHUNK, k2.shape[1]), lambda i: (i + base, 0)),
            pl.BlockSpec((CHUNK, wide), lambda i: (i + base, 0)),
            pl.BlockSpec((gates_beta.shape[0], CHUNK), lambda i: (0, i + base)),
            whole,
        ]
        + [pl.BlockSpec(memory_space=pl.ANY)] * len(earlier),
        out_specs=[
            pl.BlockSpec((CHUNK, wide), lambda i: (i + base, 0)),
            pl.BlockSpec((CHUNK, wide), lambda i: (i + base, 0)),
            whole,
            whole,
        ],
        out_shape=[
            jax.ShapeDtypeStruct((length, wide), BF16),
            jax.ShapeDtypeStruct((length, wide), F32),
            jax.ShapeDtypeStruct((units, LANES, 2 * LANES), F32),
            jax.ShapeDtypeStruct((units, LANES, 2 * LANES), BF16),
        ],
        scratch_shapes=[pltpu.VMEM((units, LANES, 2 * LANES), F32)],
        input_output_aliases={7 + i: i for i in range(len(earlier))},
        cost_estimate=pl.CostEstimate(
            flops=steps * 4 * 400 * CHUNK**3, bytes_accessed=length * wide * 10, transcendentals=0
        ),
    )(q1, k1, q2, k2, values, gates_beta, running, *earlier)


def exchange_kernel(own_ref, all_ref, send_sem, recv_sem):
    me = lax.axis_index("sp")
    count = all_ref.shape[0]
    barrier = pltpu.get_barrier_semaphore()
    for gap in range(1, count):
        pl.semaphore_signal(
            barrier,
            inc=1,
            device_id={"sp": lax.rem(me + gap, count)},
            device_id_type=pl.DeviceIdType.MESH,
        )
    pl.semaphore_wait(barrier, count - 1)

    def copy(source, target):
        return pltpu.make_async_remote_copy(
            src_ref=own_ref,
            dst_ref=all_ref.at[source],
            send_sem=send_sem.at[target],
            recv_sem=recv_sem.at[source],
            device_id={"sp": target},
            device_id_type=pl.DeviceIdType.MESH,
        )

    for target in range(1, count):
        @pl.when(me < target)
        def _():
            copy(me, target).start()

    for source in range(count - 1):
        @pl.when(source < me)
        def _():
            copy(source, me).wait_recv()

    for target in range(1, count):
        @pl.when(me < target)
        def _():
            copy(me, target).wait_send()


def exchange(summary):
    count = lax.axis_size("sp")
    return pl.pallas_call(
        exchange_kernel,
        in_specs=[pl.BlockSpec(memory_space=pltpu.VMEM)],
        out_specs=pl.BlockSpec(memory_space=pltpu.VMEM),
        out_shape=jax.ShapeDtypeStruct((count, *summary.shape), summary.dtype),
        scratch_shapes=[pltpu.SemaphoreType.DMA((count,)), pltpu.SemaphoreType.DMA((count,))],
        compiler_params=pltpu.CompilerParams(collective_id=1, has_side_effects=True),
        cost_estimate=pl.CostEstimate(flops=10**9, bytes_accessed=10**6, transcendentals=0),
    )(summary)


def swap_pair(value):
    count = lax.axis_size("sp")
    return lax.ppermute(value, "sp", [(i, i ^ 1) for i in range(count)])


def around(value, turn):
    count = lax.axis_size("sp")
    return lax.ppermute(value, "sp", [(i, (i + 2 * turn) % count) for i in range(count)])


def gather_first(own):
    near = swap_pair(own)
    return own, near, around(own, 1), around(own, -1)


def gather_rest(first):
    own, near, right, left = first
    ring = lax.axis_size("sp") // 2
    rows = own.shape[0]
    pieces = [(0, 0, 0, own), (0, 1, 0, near)]
    near_right, near_left = near, near
    for gap in range(1, (ring + 1) // 2):
        if gap > 1:
            right, left = around(right, 1), around(left, -1)
        near_right, near_left = around(near_right, 1), around(near_left, -1)
        pieces += [(gap, 0, 0, right), (ring - gap, 0, 0, left)]
        pieces += [(gap, 1, 0, near_right), (ring - gap, 1, 0, near_left)]
    if ring % 2 == 0:
        half = rows // 2
        if ring > 2:
            far_one, far_two = around(right[:half], 1), around(left[half:], -1)
        else:
            far_one, far_two = right[:half], right[half:]
        pieces += [(ring // 2, 0, 0, far_one), (ring // 2, 0, half, far_two)]
        pieces += [(ring // 2, 1, 0, swap_pair(far_one)), (ring // 2, 1, half, swap_pair(far_two))]
    return pieces


def load_pieces(meta, refs, ranges, targets, sem):
    me = lax.axis_index("sp")
    count = lax.axis_size("sp")
    ring = count // 2
    copies = []
    for (gap, other, first), ref in zip(meta, refs):
        owner = lax.rem(me // 2 + ring - gap, ring) * 2 + (lax.rem(me, 2) + other) % 2
        rows = ref.shape[0]
        for index, (low, high) in enumerate(ranges):
            a, b = max(low, first), min(high, first + rows)
            if a >= b:
                continue
            size = high - low
            copies.append(
                pltpu.make_async_copy(
                    ref.at[pl.ds(a - first, b - a), :],
                    targets[index].at[pl.ds(pl.multiple_of(owner * size + a - low, 16), b - a), :],
                    sem.at[len(copies)],
                )
            )
    return copies


def up_kernel(meta, x_ref, halo_ref, taps_ref, *rest):
    *refs, out_ref, gate_w, up_w, xs, sem = rest
    tile = x_ref.shape[0]
    step = pl.program_id(0)
    edge = halo_ref.shape[0]
    rows = gate_w.shape[0] // lax.axis_size("sp")

    @pl.when(step == 0)
    def _():
        copies = load_pieces(meta, refs, ((0, rows), (rows, 2 * rows)), (gate_w, up_w), sem)
        for one in copies:
            one.start()
        xs[:edge, :] = halo_ref[...]
        for one in copies:
            one.wait()

    @pl.when(step > 0)
    def _():
        xs[:edge, :] = xs[tile:, :]

    xs[edge:, :] = x_ref[...]
    wide = out_ref.shape[1]
    part = min(256, wide)
    for col in range(0, wide, part):
        at = slice(col, col + part)
        taken = []
        for which, w in enumerate((gate_w, up_w)):
            low = jnp.dot(xs[...], w[:, at], preferred_element_type=F32)
            low = low.astype(BF16).astype(F32)
            total = 0.0
            for tap in range(TAPS):
                moved = low[edge - TAPS + 1 + tap : edge - TAPS + 1 + tap + tile]
                total = total + taps_ref[2 * tap + which : 2 * tap + which + 1, at] * moved
            taken.append(total)
        gate, up = taken
        out_ref[:, at] = (gate / (1.0 + jnp.exp(-gate)) * up).astype(out_ref.dtype)


def up_part(features, halo, taps, pieces):
    length, width = features.shape
    wide = taps.shape[1]
    tile = min(512, length)
    meta = [p[:3] for p in pieces]
    arrays = [p[3] for p in pieces]
    edge = halo.shape[0]
    return pl.pallas_call(
        functools.partial(up_kernel, meta),
        grid=(length // tile,),
        in_specs=[
            pl.BlockSpec((tile, width), lambda i: (i, 0)),
            pl.BlockSpec(halo.shape, lambda i: (0, 0)),
            pl.BlockSpec(taps.shape, lambda i: (0, 0)),
        ]
        + [pl.BlockSpec(memory_space=pl.ANY)] * len(arrays),
        out_specs=pl.BlockSpec((tile, wide), lambda i: (i, 0)),
        out_shape=jax.ShapeDtypeStruct((length, wide), BF16),
        scratch_shapes=[
            pltpu.VMEM((width, wide), BF16),
            pltpu.VMEM((width, wide), BF16),
            pltpu.VMEM((tile + edge, width), BF16),
            pltpu.SemaphoreType.DMA((2 * len(arrays),)),
        ],
        compiler_params=pltpu.CompilerParams(vmem_limit_bytes=50 * 2**20),
        cost_estimate=pl.CostEstimate(
            flops=4 * length * width * wide, bytes_accessed=4 * width * wide, transcendentals=0
        ),
    )(features, halo, taps, *arrays)


def down_kernel(meta, x_ref, *rest):
    *refs, out_ref, down_w, sem = rest
    rows = down_w.shape[0] // lax.axis_size("sp")

    @pl.when(pl.program_id(0) == 0)
    def _():
        copies = load_pieces(meta, refs, ((0, rows),), (down_w,), sem)
        for one in copies:
            one.start()
        for one in copies:
            one.wait()

    wide = out_ref.shape[1]
    part = min(512, wide)
    for col in range(0, wide, part):
        out_ref[:, col : col + part] = mm_nt(x_ref[...], down_w[col : col + part, :]).astype(BF16)


def down_part(hidden, width, pieces):
    length, wide = hidden.shape
    tile = min(512, length)
    meta = [p[:3] for p in pieces]
    arrays = [p[3] for p in pieces]
    return pl.pallas_call(
        functools.partial(down_kernel, meta),
        grid=(length // tile,),
        in_specs=[pl.BlockSpec((tile, wide), lambda i: (i, 0))]
        + [pl.BlockSpec(memory_space=pl.ANY)] * len(arrays),
        out_specs=pl.BlockSpec((tile, width), lambda i: (i, 0)),
        out_shape=jax.ShapeDtypeStruct((length, width), BF16),
        scratch_shapes=[
            pltpu.VMEM((width, wide), BF16),
            pltpu.SemaphoreType.DMA((len(arrays),)),
        ],
        compiler_params=pltpu.CompilerParams(vmem_limit_bytes=50 * 2**20),
        cost_estimate=pl.CostEstimate(
            flops=2 * length * width * wide, bytes_accessed=2 * width * wide, transcendentals=0
        ),
    )(hidden, *arrays)


def finish_kernel(place_ref, all_ref, g_ref, h_ref, gate_ref, coef_ref, out_ref, state_ref):
    @pl.when(pl.program_id(0) == 0)
    def _():
        state_ref[...] = jnp.zeros_like(state_ref)

        def turn(i, carry):
            for unit in range(all_ref.shape[1]):
                block = all_ref[i, unit]
                state_ref[unit] = (
                    mm(block[:, LANES:], state_ref[unit]) + block[:, :LANES].astype(F32)
                )
            return carry

        lax.fori_loop(0, place_ref[0], turn, 0)

    coef = coef_ref[...]
    count = out_ref.shape[1] // LANES // 2
    for head in range(2 * count):
        unit = head if head < count else count + (head - count) // 2
        at = pl.ds(head * LANES, LANES)
        out = mm(g_ref[:, at], state_ref[unit]) + h_ref[:, at]
        gate = gate_ref[:, at].astype(F32)
        scaled = out * lax.rsqrt(jnp.mean(out * out, axis=-1, keepdims=True) + EPSILON) * coef
        out_ref[:, at] = (scaled * (gate / (1.0 + jnp.exp(-gate)))).astype(out_ref.dtype)


def finish_heads(place, everyone, g, h, gates, coef):
    length, wide = g.shape
    tile = min(256, length)
    return pl.pallas_call(
        finish_kernel,
        grid_spec=pltpu.PrefetchScalarGridSpec(
            num_scalar_prefetch=1,
            grid=(length // tile,),
            in_specs=[
                pl.BlockSpec(everyone.shape, lambda i, p: (0, 0, 0, 0)),
                pl.BlockSpec((tile, wide), lambda i, p: (i, 0)),
                pl.BlockSpec((tile, wide), lambda i, p: (i, 0)),
                pl.BlockSpec((tile, wide), lambda i, p: (i, 0)),
                pl.BlockSpec((1, LANES), lambda i, p: (0, 0)),
            ],
            out_specs=pl.BlockSpec((tile, wide), lambda i, p: (i, 0)),
            scratch_shapes=[pltpu.VMEM((everyone.shape[1], LANES, LANES), F32)],
        ),
        out_shape=jax.ShapeDtypeStruct((length, wide), BF16),
        cost_estimate=pl.CostEstimate(
            flops=2 * length * wide * LANES * 8, bytes_accessed=length * wide * 10, transcendentals=0
        ),
    )(place, everyone, g, h, gates, coef)


def per_device(
    arriving_hidden_state,
    former_request_vectors,
    former_match_vectors,
    latter_request_vectors,
    latter_match_vectors,
    stored_vectors_both,
    closing_valve_operands,
    update_level_before_squash,
    fading_data_input,
    sparse_fading_boost,
    unitwise_fading_loglevel,
    fading_constant_term,
    unitwise_normalizer_coef,
    emission_map_weights,
    channel_normalizer_coef,
    switching_channel_map,
    broadening_channel_map,
    timewise_convolve_tapvalues,
    narrowing_map_weights_in,
):
    length = former_request_vectors.shape[0]
    level = (
        -jnp.exp(unitwise_fading_loglevel)[..., None]
        * jax.nn.softplus(fading_data_input + fading_constant_term[..., None])
        + sparse_fading_boost
    )
    beta_rate = jax.nn.sigmoid(update_level_before_squash.astype(jnp.float32))
    gates_beta = jnp.concatenate([level, beta_rate], axis=0).reshape(-1, length)
    gates_beta = jnp.pad(gates_beta, ((0, -gates_beta.shape[0] % 8), (0, 0)))
    spare = -latter_request_vectors.shape[1] % LANES
    sides = jnp.concatenate([switching_channel_map, broadening_channel_map], axis=0)
    first = gather_first(sides)
    units = former_request_vectors.shape[1] // LANES + (
        latter_request_vectors.shape[1] + spare
    ) // LANES
    running = jnp.broadcast_to(jnp.eye(LANES, 2 * LANES, LANES, dtype=F32), (units, LANES, 2 * LANES))
    drawn = (
        former_request_vectors,
        former_match_vectors,
        jnp.pad(latter_request_vectors, ((0, 0), (0, spare))),
        jnp.pad(latter_match_vectors, ((0, 0), (0, spare))),
        stored_vectors_both.reshape(length, -1),
        gates_beta,
    )
    g_half, h_half, running, _ = local_terms(*drawn, running, 0, 2, ())
    running, first = lax.optimization_barrier((running, first))
    side_pieces = gather_rest(first)
    g_part, h_part, _, summary = local_terms(*drawn, running, 1, 2, (g_half, h_half))
    everyone = exchange(summary)
    everyone, narrow = lax.optimization_barrier((everyone, narrowing_map_weights_in))
    down_pieces = gather_rest(gather_first(narrow))
    place = lax.axis_index("sp").astype(jnp.int32).reshape(1)
    attended = finish_heads(
        place,
        everyone,
        g_part,
        h_part,
        closing_valve_operands.reshape(length, -1),
        unitwise_normalizer_coef.reshape(1, -1),
    )
    linear_attend = attended.reshape(length, 2, -1)
    arrived = lax.all_to_all(linear_attend, "tp", split_axis=0, concat_axis=2, tiled=True)
    row_count = arrived.shape[0]
    skip_stream = arriving_hidden_state.astype(jnp.float32) + jnp.dot(
        arrived.reshape(row_count, -1), emission_map_weights, preferred_element_type=jnp.float32
    )
    normed = (
        skip_stream
        * lax.rsqrt(jnp.mean(skip_stream * skip_stream, axis=-1, keepdims=True) + EPSILON)
        * channel_normalizer_coef
    ).astype(jnp.bfloat16)
    features = lax.all_gather(normed, "tp", axis=0, tiled=True)
    edge = 16
    halo = from_behind(features[-edge:], "sp", 1)
    taps = timewise_convolve_tapvalues.astype(F32).reshape(2 * TAPS, -1)
    hidden = up_part(features, halo, taps, side_pieces)
    down_sum = lax.psum_scatter(
        down_part(hidden, features.shape[1], down_pieces),
        "tp",
        scatter_dimension=0,
        tiled=True,
    ).astype(jnp.float32)
    return (skip_stream + down_sum).astype(jnp.bfloat16)


def solution(mesh):
    placed = (
        P(("sp", "tp"), None),
        P("sp", "tp"),
        P("sp", "tp"),
        P("sp", "tp"),
        P("sp", "tp"),
        P("sp", None, "tp"),
        P("sp", None, "tp"),
        P(None, "tp", "sp"),
        P(None, "tp", "sp"),
        P(None, "tp", "sp"),
        P(None, "tp"),
        P(None, "tp"),
        P(),
        P(),
        P(),
        P("sp", "tp"),
        P("sp", "tp"),
        P(None, None, "tp"),
        P("sp", "tp"),
    )
    return jax.shard_map(
        per_device, mesh=mesh, in_specs=placed, out_specs=P(("sp", "tp"), None), check_vma=False
    )
```

```python
import functools

import jax
import jax.numpy as jnp
from jax import lax
from jax.experimental import pallas as pl
from jax.experimental.pallas import tpu as pltpu
from jax.sharding import PartitionSpec as P


TAPS = 3
CHUNK = 128
BASE = 16
LANES = 128

EPSILON = 1e-06
F32 = jnp.float32
BF16 = jnp.bfloat16


def from_behind(value, axis, steps):
    count = lax.axis_size(axis)
    leading, last = (max(0, -steps), min(count, count - steps))
    return lax.ppermute(value, axis, [(source, source + steps) for source in range(leading, last)])


def mm(a, b):
    return jnp.dot(a.astype(BF16), b.astype(BF16), preferred_element_type=F32)


def mm_nt(a, b):
    return lax.dot_general(
        a.astype(BF16), b.astype(BF16), (((1,), (1,)), ((), ())), preferred_element_type=F32
    )


def mm_tn(a, b):
    return mm(a.T, b)


def local_kernel(
    q1_ref, k1_ref, q2_ref, k2_ref, v_ref, gb_ref, from_ref, *rest
):
    g_ref, h_ref, last_ref, sum_ref, run_ref = rest[-5:]
    step = pl.program_id(0)
    count = v_ref.shape[1] // LANES // 2
    pair = 2
    rows = lax.broadcasted_iota(jnp.int32, (CHUNK, CHUNK), 0)
    cols = lax.broadcasted_iota(jnp.int32, (CHUNK, CHUNK), 1)
    eye = (rows == cols).astype(F32)
    causal = rows >= cols
    strict = rows > cols
    lane = lax.broadcasted_iota(jnp.int32, (1, LANES), 1)

    @pl.when(step == 0)
    def _():
        run_ref[...] = from_ref[...]

    gb = gb_ref[...]
    cum = gb
    lanes8 = lax.broadcasted_iota(jnp.int32, gb.shape, 1)
    shift = 1
    while shift < CHUNK:
        cum = cum + jnp.where(lanes8 >= shift, pltpu.roll(cum, shift, 1), 0.0)
        shift *= 2
    gbt = gb.T
    cumt = cum.T

    pend = None
    for head in range(2 * count):
        group, at = head // count, head % count
        if group == 0:
            q = q1_ref[:, at * LANES : (at + 1) * LANES].astype(F32)
            k = k1_ref[:, at * LANES : (at + 1) * LANES].astype(F32)
            key_size = LANES
            own = None
        else:
            key_size = LANES // 2
            own = (lane // key_size) == at % pair
            first = (at // pair) * LANES
            q = jnp.where(own, q2_ref[:, first : first + LANES].astype(F32), 0.0)
            k = jnp.where(own, k2_ref[:, first : first + LANES].astype(F32), 0.0)
        q = q * (lax.rsqrt(jnp.sum(q * q, axis=-1, keepdims=True) + EPSILON) * key_size ** (-0.5))
        k = k * lax.rsqrt(jnp.sum(k * k, axis=-1, keepdims=True) + EPSILON)
        v = v_ref[:, head * LANES : (head + 1) * LANES].astype(F32)
        beta = gbt[:, 2 * count + head : 2 * count + head + 1]
        cum_col = cumt[:, head : head + 1]
        cum_row = cum[head : head + 1, :]
        total = cum[head : head + 1, CHUNK - 1 : CHUNK]
        decay = jnp.exp(jnp.where(causal, cum_col - cum_row, -1e30))
        grown = jnp.exp(cum_col)
        kbeta = k * beta
        kbf = k.astype(BF16)
        low = jnp.where(strict, mm_nt(kbeta, kbf) * decay, 0.0)
        intra = mm_nt(q, kbf) * decay
        base = jnp.where((rows // BASE) == (cols // BASE), low, 0.0)
        power = -base
        inv = eye + power
        size = 2
        while size < BASE:
            power = mm(power, power)
            inv = inv + mm(inv, power)
            size *= 2
        block = BASE
        while block < CHUNK:
            off = jnp.where(
                ((rows // (2 * block)) == (cols // (2 * block)))
                & ((rows // block) != (cols // block)),
                low,
                0.0,
            )
            inv = inv - mm(mm(inv, off), inv)
            block *= 2
        right = jnp.concatenate([v * beta, kbeta * grown], axis=-1)
        solved = mm(inv, right)
        kdec = k * jnp.exp(total - cum_col)
        both = mm_tn(kdec, solved)
        inner = mm(intra, solved)
        unit_diag = eye if own is None else jnp.where(own, eye, 0.0)
        cmap = jnp.exp(total) * unit_diag - both[:, LANES:]
        cadd = both[:, :LANES]
        pmat = q * grown - inner[:, LANES:]
        unit = head if group == 0 else count + at // pair
        run = run_ref[unit]
        seen = mm(pmat, run)
        h_ref[:, head * LANES : (head + 1) * LANES] = seen[:, :LANES] + inner[:, :LANES]
        g_ref[:, head * LANES : (head + 1) * LANES] = seen[:, LANES:].astype(g_ref.dtype)
        if pend is not None:
            cmap = cmap + pend[0]
            cadd = cadd + pend[1]
            pend = None
        if group == 1 and at % pair != pair - 1 and at != count - 1:
            pend = (cmap, cadd)
            continue
        nxt = mm(cmap, run)
        run_ref[unit, :, :LANES] = nxt[:, :LANES] + cadd
        run_ref[unit, :, LANES:] = nxt[:, LANES:]

    @pl.when(step == pl.num_programs(0) - 1)
    def _():
        last_ref[...] = run_ref[...]
        sum_ref[...] = run_ref[...].astype(sum_ref.dtype)


def local_terms(q1, k1, q2, k2, values, gates_beta, running, part, parts, earlier):
    length = q1.shape[0]
    wide = values.shape[1]
    steps = length // CHUNK // parts
    base = part * steps
    units = running.shape[0]
    whole = pl.BlockSpec((units, LANES, 2 * LANES), lambda i: (0, 0, 0))
    return pl.pallas_call(
        local_kernel,
        grid=(steps,),
        in_specs=[
            pl.BlockSpec((CHUNK, q1.shape[1]), lambda i: (i + base, 0)),
            pl.BlockSpec((CHUNK, k1.shape[1]), lambda i: (i + base, 0)),
            pl.BlockSpec((CHUNK, q2.shape[1]), lambda i: (i + base, 0)),
            pl.BlockSpec((CHUNK, k2.shape[1]), lambda i: (i + base, 0)),
            pl.BlockSpec((CHUNK, wide), lambda i: (i + base, 0)),
            pl.BlockSpec((gates_beta.shape[0], CHUNK), lambda i: (0, i + base)),
            whole,
        ]
        + [pl.BlockSpec(memory_space=pl.ANY)] * len(earlier),
        out_specs=[
            pl.BlockSpec((CHUNK, wide), lambda i: (i + base, 0)),
            pl.BlockSpec((CHUNK, wide), lambda i: (i + base, 0)),
            whole,
            whole,
        ],
        out_shape=[
            jax.ShapeDtypeStruct((length, wide), BF16),
            jax.ShapeDtypeStruct((length, wide), F32),
            jax.ShapeDtypeStruct((units, LANES, 2 * LANES), F32),
            jax.ShapeDtypeStruct((units, LANES, 2 * LANES), BF16),
        ],
        scratch_shapes=[pltpu.VMEM((units, LANES, 2 * LANES), F32)],
        input_output_aliases={7 + i: i for i in range(len(earlier))},
        cost_estimate=pl.CostEstimate(
            flops=steps * 4 * 400 * CHUNK**3, bytes_accessed=length * wide * 10, transcendentals=0
        ),
    )(q1, k1, q2, k2, values, gates_beta, running, *earlier)


def exchange_kernel(own_ref, all_ref, send_sem, recv_sem):
    me = lax.axis_index("sp")
    count = all_ref.shape[0]
    barrier = pltpu.get_barrier_semaphore()
    for gap in range(1, count):
        pl.semaphore_signal(
            barrier,
            inc=1,
            device_id={"sp": lax.rem(me + gap, count)},
            device_id_type=pl.DeviceIdType.MESH,
        )
    pl.semaphore_wait(barrier, count - 1)

    def copy(source, target):
        return pltpu.make_async_remote_copy(
            src_ref=own_ref,
            dst_ref=all_ref.at[source],
            send_sem=send_sem.at[target],
            recv_sem=recv_sem.at[source],
            device_id={"sp": target},
            device_id_type=pl.DeviceIdType.MESH,
        )

    for target in range(1, count):
        @pl.when(me < target)
        def _():
            copy(me, target).start()

    for source in range(count - 1):
        @pl.when(source < me)
        def _():
            copy(source, me).wait_recv()

    for target in range(1, count):
        @pl.when(me < target)
        def _():
            copy(me, target).wait_send()


def exchange(summary):
    count = lax.axis_size("sp")
    return pl.pallas_call(
        exchange_kernel,
        in_specs=[pl.BlockSpec(memory_space=pltpu.VMEM)],
        out_specs=pl.BlockSpec(memory_space=pltpu.VMEM),
        out_shape=jax.ShapeDtypeStruct((count, *summary.shape), summary.dtype),
        scratch_shapes=[pltpu.SemaphoreType.DMA((count,)), pltpu.SemaphoreType.DMA((count,))],
        compiler_params=pltpu.CompilerParams(collective_id=1, has_side_effects=True),
        cost_estimate=pl.CostEstimate(flops=10**9, bytes_accessed=10**6, transcendentals=0),
    )(summary)


def swapped(value, low, high):
    places = [2 * place + parity for place in range(low, high) for parity in range(2)]
    return lax.ppermute(value, "sp", [(i, i ^ 1) for i in places])


def line_start(own):
    ring = lax.axis_size("sp") // 2
    return dict(
        right=own, left=own, pieces=[(0, 0, 0, ring, own), (0, 1, 0, ring, swapped(own, 0, ring))]
    )


def line_step(line, gap):
    ring = lax.axis_size("sp") // 2
    if gap >= ring:
        return line
    up = [(2 * p + q, 2 * p + 2 + q) for p in range(gap - 1, ring - 1) for q in range(2)]
    down = [(2 * p + q, 2 * p - 2 + q) for p in range(1, ring - gap + 1) for q in range(2)]
    right = lax.ppermute(line["right"], "sp", up)
    left = lax.ppermute(line["left"], "sp", down)
    pieces = [(gap, 0, gap, ring, right), (ring - gap, 0, 0, ring - gap, left)]
    return dict(right=right, left=left, pieces=line["pieces"] + pieces)


def line_swap(line, gap):
    ring = lax.axis_size("sp") // 2
    if gap >= ring:
        return line
    pieces = [
        (gap, 1, gap, ring, swapped(line["right"], gap, ring)),
        (ring - gap, 1, 0, ring - gap, swapped(line["left"], 0, ring - gap)),
    ]
    return dict(line, pieces=line["pieces"] + pieces)


def line_rest(line, gap):
    ring = lax.axis_size("sp") // 2
    for more in range(gap, ring):
        line = line_swap(line_step(line, more), more)
    return line


def tie(line, other):
    other, right, left = lax.optimization_barrier((other, line["right"], line["left"]))
    return dict(line, right=right, left=left), other


def load_pieces(meta, refs, ranges, targets, sem):
    me = lax.axis_index("sp")
    ring = lax.axis_size("sp") // 2
    place = me // 2
    copies = []
    for (gap, other, low_place, high_place), ref in zip(meta, refs):
        owner = lax.rem(place + ring - gap, ring) * 2 + (lax.rem(me, 2) + other) % 2
        valid = (place >= low_place) & (place < high_place)
        for index, (low, high) in enumerate(ranges):
            size = high - low
            one = pltpu.make_async_copy(
                ref.at[pl.ds(low, size), :],
                targets[index].at[pl.ds(pl.multiple_of(owner * size, 16), size), :],
                sem.at[len(copies)],
            )
            copies.append((valid, one))

    for valid, one in copies:
        @pl.when(valid)
        def _():
            one.start()

    return copies


def finish_pieces(copies):
    for valid, one in copies:
        @pl.when(valid)
        def _():
            one.wait()


def project_kernel(x_ref, w_ref, skip_ref, coef_ref, sum_ref, out_ref):
    step = pl.program_id(0)

    @pl.when(step == 0)
    def _():
        sum_ref[...] = skip_ref[...].astype(F32)

    sum_ref[...] += jnp.dot(x_ref[...], w_ref[...], preferred_element_type=F32)

    @pl.when(step == pl.num_programs(0) - 1)
    def _():
        total = sum_ref[...]
        scale = lax.rsqrt(jnp.mean(total * total, axis=-1, keepdims=True) + EPSILON)
        out_ref[...] = (total * scale * coef_ref[...]).astype(out_ref.dtype)


def project(x, weights, skip, coef):
    rows, depth = x.shape
    width = weights.shape[1]
    part = min(512, depth)
    whole = pl.BlockSpec((rows, width), lambda i: (0, 0))
    return pl.pallas_call(
        project_kernel,
        grid=(depth // part,),
        in_specs=[
            pl.BlockSpec((rows, part), lambda i: (0, i)),
            pl.BlockSpec((part, width), lambda i: (i, 0)),
            whole,
            pl.BlockSpec((1, width), lambda i: (0, 0)),
        ],
        out_specs=[whole, whole],
        out_shape=[
            jax.ShapeDtypeStruct((rows, width), F32),
            jax.ShapeDtypeStruct((rows, width), BF16),
        ],
        cost_estimate=pl.CostEstimate(
            flops=2 * rows * depth * width, bytes_accessed=2 * depth * width, transcendentals=0
        ),
    )(x, weights, skip, coef)


def up_kernel(meta, x_ref, halo_ref, taps_ref, *rest):
    *refs, out_ref, gate_w, up_w, xs, sem = rest
    tile = x_ref.shape[0]
    step = pl.program_id(0)
    edge = halo_ref.shape[0]
    rows = gate_w.shape[0] // lax.axis_size("sp")

    @pl.when(step == 0)
    def _():
        copies = load_pieces(meta, refs, ((0, rows), (rows, 2 * rows)), (gate_w, up_w), sem)
        xs[:edge, :] = halo_ref[...]
        finish_pieces(copies)

    @pl.when(step > 0)
    def _():
        xs[:edge, :] = xs[tile:, :]

    xs[edge:, :] = x_ref[...]
    wide = out_ref.shape[1]
    part = min(256, wide)
    for col in range(0, wide, part):
        at = slice(col, col + part)
        taken = []
        for which, w in enumerate((gate_w, up_w)):
            low = jnp.dot(xs[...], w[:, at], preferred_element_type=F32)
            low = low.astype(BF16).astype(F32)
            total = 0.0
            for tap in range(TAPS):
                moved = low[edge - TAPS + 1 + tap : edge - TAPS + 1 + tap + tile]
                total = total + taps_ref[2 * tap + which : 2 * tap + which + 1, at] * moved
            taken.append(total)
        gate, up = taken
        out_ref[:, at] = (gate / (1.0 + jnp.exp(-gate)) * up).astype(out_ref.dtype)


def up_part(features, halo, taps, pieces):
    length, width = features.shape
    wide = taps.shape[1]
    tile = min(512, length)
    meta = [p[:4] for p in pieces]
    arrays = [p[4] for p in pieces]
    edge = halo.shape[0]
    return pl.pallas_call(
        functools.partial(up_kernel, meta),
        grid=(length // tile,),
        in_specs=[
            pl.BlockSpec((tile, width), lambda i: (i, 0)),
            pl.BlockSpec(halo.shape, lambda i: (0, 0)),
            pl.BlockSpec(taps.shape, lambda i: (0, 0)),
        ]
        + [pl.BlockSpec(memory_space=pl.ANY)] * len(arrays),
        out_specs=pl.BlockSpec((tile, wide), lambda i: (i, 0)),
        out_shape=jax.ShapeDtypeStruct((length, wide), BF16),
        scratch_shapes=[
            pltpu.VMEM((width, wide), BF16),
            pltpu.VMEM((width, wide), BF16),
            pltpu.VMEM((tile + edge, width), BF16),
            pltpu.SemaphoreType.DMA((2 * len(arrays),)),
        ],
        compiler_params=pltpu.CompilerParams(vmem_limit_bytes=50 * 2**20),
        cost_estimate=pl.CostEstimate(
            flops=4 * length * width * wide, bytes_accessed=4 * width * wide, transcendentals=0
        ),
    )(features, halo, taps, *arrays)


def down_kernel(meta, x_ref, *rest):
    *refs, out_ref, down_w, sem = rest
    rows = down_w.shape[0] // lax.axis_size("sp")

    @pl.when(pl.program_id(0) == 0)
    def _():
        copies = load_pieces(meta, refs, ((0, rows),), (down_w,), sem)
        finish_pieces(copies)

    wide = out_ref.shape[1]
    part = min(512, wide)
    for col in range(0, wide, part):
        out_ref[:, col : col + part] = mm_nt(x_ref[...], down_w[col : col + part, :]).astype(BF16)


def down_part(hidden, width, pieces):
    length, wide = hidden.shape
    tile = min(512, length)
    meta = [p[:4] for p in pieces]
    arrays = [p[4] for p in pieces]
    return pl.pallas_call(
        functools.partial(down_kernel, meta),
        grid=(length // tile,),
        in_specs=[pl.BlockSpec((tile, wide), lambda i: (i, 0))]
        + [pl.BlockSpec(memory_space=pl.ANY)] * len(arrays),
        out_specs=pl.BlockSpec((tile, width), lambda i: (i, 0)),
        out_shape=jax.ShapeDtypeStruct((length, width), BF16),
        scratch_shapes=[
            pltpu.VMEM((width, wide), BF16),
            pltpu.SemaphoreType.DMA((len(arrays),)),
        ],
        compiler_params=pltpu.CompilerParams(vmem_limit_bytes=50 * 2**20),
        cost_estimate=pl.CostEstimate(
            flops=2 * length * width * wide, bytes_accessed=2 * width * wide, transcendentals=0
        ),
    )(hidden, *arrays)


def finish_kernel(place_ref, all_ref, g_ref, h_ref, gate_ref, coef_ref, out_ref, state_ref):
    @pl.when(pl.program_id(0) == 0)
    def _():
        state_ref[...] = jnp.zeros_like(state_ref)

        def turn(i, carry):
            for unit in range(all_ref.shape[1]):
                block = all_ref[i, unit]
                state_ref[unit] = (
                    mm(block[:, LANES:], state_ref[unit]) + block[:, :LANES].astype(F32)
                )
            return carry

        lax.fori_loop(0, place_ref[0], turn, 0)

    coef = coef_ref[...]
    count = out_ref.shape[1] // LANES // 2
    for head in range(2 * count):
        unit = head if head < count else count + (head - count) // 2
        at = pl.ds(head * LANES, LANES)
        out = mm(g_ref[:, at], state_ref[unit]) + h_ref[:, at]
        gate = gate_ref[:, at].astype(F32)
        scaled = out * lax.rsqrt(jnp.mean(out * out, axis=-1, keepdims=True) + EPSILON) * coef
        out_ref[:, at] = (scaled * (gate / (1.0 + jnp.exp(-gate)))).astype(out_ref.dtype)


def finish_heads(place, everyone, g, h, gates, coef):
    length, wide = g.shape
    tile = min(256, length)
    return pl.pallas_call(
        finish_kernel,
        grid_spec=pltpu.PrefetchScalarGridSpec(
            num_scalar_prefetch=1,
            grid=(length // tile,),
            in_specs=[
                pl.BlockSpec(everyone.shape, lambda i, p: (0, 0, 0, 0)),
                pl.BlockSpec((tile, wide), lambda i, p: (i, 0)),
                pl.BlockSpec((tile, wide), lambda i, p: (i, 0)),
                pl.BlockSpec((tile, wide), lambda i, p: (i, 0)),
                pl.BlockSpec((1, LANES), lambda i, p: (0, 0)),
            ],
            out_specs=pl.BlockSpec((tile, wide), lambda i, p: (i, 0)),
            scratch_shapes=[pltpu.VMEM((everyone.shape[1], LANES, LANES), F32)],
        ),
        out_shape=jax.ShapeDtypeStruct((length, wide), BF16),
        cost_estimate=pl.CostEstimate(
            flops=2 * length * wide * LANES * 8, bytes_accessed=length * wide * 10, transcendentals=0
        ),
    )(place, everyone, g, h, gates, coef)


def per_device(
    arriving_hidden_state,
    former_request_vectors,
    former_match_vectors,
    latter_request_vectors,
    latter_match_vectors,
    stored_vectors_both,
    closing_valve_operands,
    update_level_before_squash,
    fading_data_input,
    sparse_fading_boost,
    unitwise_fading_loglevel,
    fading_constant_term,
    unitwise_normalizer_coef,
    emission_map_weights,
    channel_normalizer_coef,
    switching_channel_map,
    broadening_channel_map,
    timewise_convolve_tapvalues,
    narrowing_map_weights_in,
):
    length = former_request_vectors.shape[0]
    level = (
        -jnp.exp(unitwise_fading_loglevel)[..., None]
        * jax.nn.softplus(fading_data_input + fading_constant_term[..., None])
        + sparse_fading_boost
    )
    beta_rate = jax.nn.sigmoid(update_level_before_squash.astype(jnp.float32))
    gates_beta = jnp.concatenate([level, beta_rate], axis=0).reshape(-1, length)
    gates_beta = jnp.pad(gates_beta, ((0, -gates_beta.shape[0] % 8), (0, 0)))
    spare = -latter_request_vectors.shape[1] % LANES
    sides = jnp.concatenate([switching_channel_map, broadening_channel_map], axis=0)
    side = line_step(line_start(sides), 1)
    units = former_request_vectors.shape[1] // LANES + (
        latter_request_vectors.shape[1] + spare
    ) // LANES
    running = jnp.broadcast_to(jnp.eye(LANES, 2 * LANES, LANES, dtype=F32), (units, LANES, 2 * LANES))
    drawn = (
        former_request_vectors,
        former_match_vectors,
        jnp.pad(latter_request_vectors, ((0, 0), (0, spare))),
        jnp.pad(latter_match_vectors, ((0, 0), (0, spare))),
        stored_vectors_both.reshape(length, -1),
        gates_beta,
    )
    parts = 4 if length % (4 * CHUNK) == 0 else 1
    done = ()
    summary = None
    for part in range(parts):
        if part == parts // 2:
            side, running = tie(side, running)
            side = line_step(line_swap(side, 1), 2)
        *done, running, summary = local_terms(*drawn, running, part, parts, tuple(done))
    g_part, h_part = done
    everyone = exchange(summary)
    side, (everyone, narrow) = tie(side, (everyone, narrowing_map_weights_in))
    side = line_step(line_swap(side, 2), 3)
    down = line_step(line_start(narrow), 1)
    place = lax.axis_index("sp").astype(jnp.int32).reshape(1)
    attended = finish_heads(
        place,
        everyone,
        g_part,
        h_part,
        closing_valve_operands.reshape(length, -1),
        unitwise_normalizer_coef.reshape(1, -1),
    )
    linear_attend = attended.reshape(length, 2, -1)
    arrived = lax.all_to_all(linear_attend, "tp", split_axis=0, concat_axis=2, tiled=True)
    row_count = arrived.shape[0]
    skip_stream, normed = project(
        arrived.reshape(row_count, -1),
        emission_map_weights,
        arriving_hidden_state,
        channel_normalizer_coef.reshape(1, -1),
    )
    side, normed = tie(side, normed)
    side = line_rest(line_swap(side, 3), 4)
    features = lax.all_gather(normed, "tp", axis=0, tiled=True)
    down = line_step(line_swap(down, 1), 2)
    edge = 16
    halo = from_behind(features[-edge:], "sp", 1)
    taps = timewise_convolve_tapvalues.astype(F32).reshape(2 * TAPS, -1)
    down, halo = tie(down, halo)
    down = line_step(line_swap(down, 2), 3)
    hidden = up_part(features, halo, taps, side["pieces"])
    down = line_rest(line_swap(down, 3), 4)
    down_sum = lax.psum_scatter(
        down_part(hidden, features.shape[1], down["pieces"]),
        "tp",
        scatter_dimension=0,
        tiled=True,
    ).astype(jnp.float32)
    return (skip_stream + down_sum).astype(jnp.bfloat16)


def solution(mesh):
    placed = (
        P(("sp", "tp"), None),
        P("sp", "tp"),
        P("sp", "tp"),
        P("sp", "tp"),
        P("sp", "tp"),
        P("sp", None, "tp"),
        P("sp", None, "tp"),
        P(None, "tp", "sp"),
        P(None, "tp", "sp"),
        P(None, "tp", "sp"),
        P(None, "tp"),
        P(None, "tp"),
        P(),
        P(),
        P(),
        P("sp", "tp"),
        P("sp", "tp"),
        P(None, None, "tp"),
        P("sp", "tp"),
    )
    return jax.shard_map(
        per_device, mesh=mesh, in_specs=placed, out_specs=P(("sp", "tp"), None), check_vma=False
    )
```

```python
import functools

import jax
import jax.numpy as jnp
from jax import lax
from jax.experimental import pallas as pl
from jax.experimental.pallas import tpu as pltpu
from jax.sharding import PartitionSpec as P


TAPS = 3
CHUNK = 128
BASE = 16
LANES = 128

EPSILON = 1e-06
F32 = jnp.float32
BF16 = jnp.bfloat16


def from_behind(value, axis, steps):
    count = lax.axis_size(axis)
    leading, last = (max(0, -steps), min(count, count - steps))
    return lax.ppermute(value, axis, [(source, source + steps) for source in range(leading, last)])


def mm(a, b):
    return jnp.dot(a.astype(BF16), b.astype(BF16), preferred_element_type=F32)


def mm_nt(a, b):
    return lax.dot_general(
        a.astype(BF16), b.astype(BF16), (((1,), (1,)), ((), ())), preferred_element_type=F32
    )


def mm_tn(a, b):
    return mm(a.T, b)


def local_kernel(
    q1_ref, k1_ref, q2_ref, k2_ref, v_ref, gb_ref, from_ref, *rest
):
    g_ref, h_ref, last_ref, sum_ref, run_ref = rest[-5:]
    step = pl.program_id(0)
    count = v_ref.shape[1] // LANES // 2
    pair = 2
    rows = lax.broadcasted_iota(jnp.int32, (CHUNK, CHUNK), 0)
    cols = lax.broadcasted_iota(jnp.int32, (CHUNK, CHUNK), 1)
    eye = (rows == cols).astype(F32)
    causal = rows >= cols
    strict = rows > cols
    lane = lax.broadcasted_iota(jnp.int32, (1, LANES), 1)

    @pl.when(step == 0)
    def _():
        run_ref[...] = from_ref[...]

    gb = gb_ref[...]
    cum = gb
    lanes8 = lax.broadcasted_iota(jnp.int32, gb.shape, 1)
    shift = 1
    while shift < CHUNK:
        cum = cum + jnp.where(lanes8 >= shift, pltpu.roll(cum, shift, 1), 0.0)
        shift *= 2
    gbt = gb.T
    cumt = cum.T

    pend = None
    for head in range(2 * count):
        group, at = head // count, head % count
        if group == 0:
            q = q1_ref[:, at * LANES : (at + 1) * LANES].astype(F32)
            k = k1_ref[:, at * LANES : (at + 1) * LANES].astype(F32)
            key_size = LANES
            own = None
        else:
            key_size = LANES // 2
            own = (lane // key_size) == at % pair
            first = (at // pair) * LANES
            q = jnp.where(own, q2_ref[:, first : first + LANES].astype(F32), 0.0)
            k = jnp.where(own, k2_ref[:, first : first + LANES].astype(F32), 0.0)
        q = q * (lax.rsqrt(jnp.sum(q * q, axis=-1, keepdims=True) + EPSILON) * key_size ** (-0.5))
        k = k * lax.rsqrt(jnp.sum(k * k, axis=-1, keepdims=True) + EPSILON)
        v = v_ref[:, head * LANES : (head + 1) * LANES].astype(F32)
        beta = gbt[:, 2 * count + head : 2 * count + head + 1]
        cum_col = cumt[:, head : head + 1]
        cum_row = cum[head : head + 1, :]
        total = cum[head : head + 1, CHUNK - 1 : CHUNK]
        decay = jnp.exp(jnp.where(causal, cum_col - cum_row, -1e30))
        grown = jnp.exp(cum_col)
        kbeta = k * beta
        kbf = k.astype(BF16)
        low = jnp.where(strict, mm_nt(kbeta, kbf) * decay, 0.0)
        intra = mm_nt(q, kbf) * decay
        base = jnp.where((rows // BASE) == (cols // BASE), low, 0.0)
        power = -base
        inv = eye + power
        size = 2
        while size < BASE:
            power = mm(power, power)
            inv = inv + mm(inv, power)
            size *= 2
        block = BASE
        while block < CHUNK:
            off = jnp.where(
                ((rows // (2 * block)) == (cols // (2 * block)))
                & ((rows // block) != (cols // block)),
                low,
                0.0,
            )
            inv = inv - mm(mm(inv, off), inv)
            block *= 2
        right = jnp.concatenate([v * beta, kbeta * grown], axis=-1)
        solved = mm(inv, right)
        kdec = k * jnp.exp(total - cum_col)
        both = mm_tn(kdec, solved)
        inner = mm(intra, solved)
        unit_diag = eye if own is None else jnp.where(own, eye, 0.0)
        cmap = jnp.exp(total) * unit_diag - both[:, LANES:]
        cadd = both[:, :LANES]
        pmat = q * grown - inner[:, LANES:]
        unit = head if group == 0 else count + at // pair
        run = run_ref[unit]
        seen = mm(pmat, run)
        h_ref[:, head * LANES : (head + 1) * LANES] = seen[:, :LANES] + inner[:, :LANES]
        g_ref[:, head * LANES : (head + 1) * LANES] = seen[:, LANES:].astype(g_ref.dtype)
        if pend is not None:
            cmap = cmap + pend[0]
            cadd = cadd + pend[1]
            pend = None
        if group == 1 and at % pair != pair - 1 and at != count - 1:
            pend = (cmap, cadd)
            continue
        nxt = mm(cmap, run)
        run_ref[unit, :, :LANES] = nxt[:, :LANES] + cadd
        run_ref[unit, :, LANES:] = nxt[:, LANES:]

    @pl.when(step == pl.num_programs(0) - 1)
    def _():
        last_ref[...] = run_ref[...]
        sum_ref[...] = run_ref[...].astype(sum_ref.dtype)


def local_terms(q1, k1, q2, k2, values, gates_beta, running, part, parts, earlier):
    length = q1.shape[0]
    wide = values.shape[1]
    steps = length // CHUNK // parts
    base = part * steps
    units = running.shape[0]
    whole = pl.BlockSpec((units, LANES, 2 * LANES), lambda i: (0, 0, 0))
    return pl.pallas_call(
        local_kernel,
        grid=(steps,),
        in_specs=[
            pl.BlockSpec((CHUNK, q1.shape[1]), lambda i: (i + base, 0)),
            pl.BlockSpec((CHUNK, k1.shape[1]), lambda i: (i + base, 0)),
            pl.BlockSpec((CHUNK, q2.shape[1]), lambda i: (i + base, 0)),
            pl.BlockSpec((CHUNK, k2.shape[1]), lambda i: (i + base, 0)),
            pl.BlockSpec((CHUNK, wide), lambda i: (i + base, 0)),
            pl.BlockSpec((gates_beta.shape[0], CHUNK), lambda i: (0, i + base)),
            whole,
        ]
        + [pl.BlockSpec(memory_space=pl.ANY)] * len(earlier),
        out_specs=[
            pl.BlockSpec((CHUNK, wide), lambda i: (i + base, 0)),
            pl.BlockSpec((CHUNK, wide), lambda i: (i + base, 0)),
            whole,
            whole,
        ],
        out_shape=[
            jax.ShapeDtypeStruct((length, wide), BF16),
            jax.ShapeDtypeStruct((length, wide), F32),
            jax.ShapeDtypeStruct((units, LANES, 2 * LANES), F32),
            jax.ShapeDtypeStruct((units, LANES, 2 * LANES), BF16),
        ],
        scratch_shapes=[pltpu.VMEM((units, LANES, 2 * LANES), F32)],
        input_output_aliases={7 + i: i for i in range(len(earlier))},
        cost_estimate=pl.CostEstimate(
            flops=steps * 4 * 400 * CHUNK**3, bytes_accessed=length * wide * 10, transcendentals=0
        ),
    )(q1, k1, q2, k2, values, gates_beta, running, *earlier)


def exchange_kernel(own_ref, all_ref, send_sem, recv_sem):
    me = lax.axis_index("sp")
    count = all_ref.shape[0]
    barrier = pltpu.get_barrier_semaphore()
    for gap in range(1, count):
        pl.semaphore_signal(
            barrier,
            inc=1,
            device_id={"sp": lax.rem(me + gap, count)},
            device_id_type=pl.DeviceIdType.MESH,
        )
    pl.semaphore_wait(barrier, count - 1)

    def copy(source, target):
        return pltpu.make_async_remote_copy(
            src_ref=own_ref,
            dst_ref=all_ref.at[source],
            send_sem=send_sem.at[target],
            recv_sem=recv_sem.at[source],
            device_id={"sp": target},
            device_id_type=pl.DeviceIdType.MESH,
        )

    for target in range(1, count):
        @pl.when(me < target)
        def _():
            copy(me, target).start()

    for source in range(count - 1):
        @pl.when(source < me)
        def _():
            copy(source, me).wait_recv()

    for target in range(1, count):
        @pl.when(me < target)
        def _():
            copy(me, target).wait_send()


def exchange(summary):
    count = lax.axis_size("sp")
    return pl.pallas_call(
        exchange_kernel,
        in_specs=[pl.BlockSpec(memory_space=pltpu.VMEM)],
        out_specs=pl.BlockSpec(memory_space=pltpu.VMEM),
        out_shape=jax.ShapeDtypeStruct((count, *summary.shape), summary.dtype),
        scratch_shapes=[pltpu.SemaphoreType.DMA((count,)), pltpu.SemaphoreType.DMA((count,))],
        compiler_params=pltpu.CompilerParams(collective_id=1, has_side_effects=True),
        cost_estimate=pl.CostEstimate(flops=10**9, bytes_accessed=10**6, transcendentals=0),
    )(summary)


def swapped(value, low, high):
    places = [2 * place + parity for place in range(low, high) for parity in range(2)]
    return lax.ppermute(value, "sp", [(i, i ^ 1) for i in places])


def line_start(own):
    ring = lax.axis_size("sp") // 2
    return dict(
        right=own, left=own, pieces=[(0, 0, 0, ring, own), (0, 1, 0, ring, swapped(own, 0, ring))]
    )


def line_step(line, gap):
    ring = lax.axis_size("sp") // 2
    if gap >= ring:
        return line
    up = [(2 * p + q, 2 * p + 2 + q) for p in range(gap - 1, ring - 1) for q in range(2)]
    down = [(2 * p + q, 2 * p - 2 + q) for p in range(1, ring - gap + 1) for q in range(2)]
    right = lax.ppermute(line["right"], "sp", up)
    left = lax.ppermute(line["left"], "sp", down)
    pieces = [(gap, 0, gap, ring, right), (ring - gap, 0, 0, ring - gap, left)]
    return dict(right=right, left=left, pieces=line["pieces"] + pieces)


def line_swap(line, gap):
    ring = lax.axis_size("sp") // 2
    if gap >= ring:
        return line
    pieces = [
        (gap, 1, gap, ring, swapped(line["right"], gap, ring)),
        (ring - gap, 1, 0, ring - gap, swapped(line["left"], 0, ring - gap)),
    ]
    return dict(line, pieces=line["pieces"] + pieces)


def line_rest(line, gap):
    ring = lax.axis_size("sp") // 2
    for more in range(gap, ring):
        line = line_swap(line_step(line, more), more)
    return line


def tie(line, other):
    other, right, left = lax.optimization_barrier((other, line["right"], line["left"]))
    return dict(line, right=right, left=left), other


def load_pieces(meta, refs, ranges, targets, sem):
    me = lax.axis_index("sp")
    ring = lax.axis_size("sp") // 2
    place = me // 2
    copies = []
    for (gap, other, low_place, high_place), ref in zip(meta, refs):
        owner = lax.rem(place + ring - gap, ring) * 2 + (lax.rem(me, 2) + other) % 2
        valid = (place >= low_place) & (place < high_place)
        for index, (low, high) in enumerate(ranges):
            size = high - low
            one = pltpu.make_async_copy(
                ref.at[pl.ds(low, size), :],
                targets[index].at[pl.ds(pl.multiple_of(owner * size, 16), size), :],
                sem.at[len(copies)],
            )
            copies.append((valid, one))

    for valid, one in copies:
        @pl.when(valid)
        def _():
            one.start()

    return copies


def finish_pieces(copies):
    for valid, one in copies:
        @pl.when(valid)
        def _():
            one.wait()


def project_kernel(x_ref, w_ref, skip_ref, coef_ref, sum_ref, out_ref):
    step = pl.program_id(0)

    @pl.when(step == 0)
    def _():
        sum_ref[...] = skip_ref[...].astype(F32)

    sum_ref[...] += jnp.dot(x_ref[0], w_ref[...], preferred_element_type=F32)

    @pl.when(step == pl.num_programs(0) - 1)
    def _():
        total = sum_ref[...]
        scale = lax.rsqrt(jnp.mean(total * total, axis=-1, keepdims=True) + EPSILON)
        out_ref[...] = (total * scale * coef_ref[...]).astype(out_ref.dtype)


def project(x, weights, skip, coef):
    team, rows, wide = x.shape
    depth, width = weights.shape
    part = wide // 2
    whole = pl.BlockSpec((rows, width), lambda i: (0, 0))
    return pl.pallas_call(
        project_kernel,
        grid=(depth // part,),
        in_specs=[
            pl.BlockSpec((1, rows, part), lambda i: (i // 2, 0, i % 2)),
            pl.BlockSpec((part, width), lambda i: ((i % 2) * team + i // 2, 0)),
            whole,
            pl.BlockSpec((1, width), lambda i: (0, 0)),
        ],
        out_specs=[whole, whole],
        out_shape=[
            jax.ShapeDtypeStruct((rows, width), F32),
            jax.ShapeDtypeStruct((rows, width), BF16),
        ],
        cost_estimate=pl.CostEstimate(
            flops=2 * rows * depth * width, bytes_accessed=2 * depth * width, transcendentals=0
        ),
    )(x, weights, skip, coef)


def up_kernel(meta, x_ref, halo_ref, taps_ref, *rest):
    *refs, out_ref, gate_w, up_w, xs, sem = rest
    tile = x_ref.shape[0]
    step = pl.program_id(0)
    edge = halo_ref.shape[0]
    rows = gate_w.shape[0] // lax.axis_size("sp")

    @pl.when(step == 0)
    def _():
        copies = load_pieces(meta, refs, ((0, rows), (rows, 2 * rows)), (gate_w, up_w), sem)
        xs[:edge, :] = halo_ref[...]
        finish_pieces(copies)

    @pl.when(step > 0)
    def _():
        xs[:edge, :] = xs[tile:, :]

    xs[edge:, :] = x_ref[...]
    wide = out_ref.shape[1]
    part = min(256, wide)
    for col in range(0, wide, part):
        at = slice(col, col + part)
        taken = []
        for which, w in enumerate((gate_w, up_w)):
            low = jnp.dot(xs[...], w[:, at], preferred_element_type=F32)
            low = low.astype(BF16).astype(F32)
            total = 0.0
            for tap in range(TAPS):
                moved = low[edge - TAPS + 1 + tap : edge - TAPS + 1 + tap + tile]
                total = total + taps_ref[2 * tap + which : 2 * tap + which + 1, at] * moved
            taken.append(total)
        gate, up = taken
        out_ref[:, at] = (gate / (1.0 + jnp.exp(-gate)) * up).astype(out_ref.dtype)


def up_part(features, halo, taps, pieces):
    length, width = features.shape
    wide = taps.shape[1]
    tile = min(512, length)
    meta = [p[:4] for p in pieces]
    arrays = [p[4] for p in pieces]
    edge = halo.shape[0]
    return pl.pallas_call(
        functools.partial(up_kernel, meta),
        grid=(length // tile,),
        in_specs=[
            pl.BlockSpec((tile, width), lambda i: (i, 0)),
            pl.BlockSpec(halo.shape, lambda i: (0, 0)),
            pl.BlockSpec(taps.shape, lambda i: (0, 0)),
        ]
        + [pl.BlockSpec(memory_space=pl.ANY)] * len(arrays),
        out_specs=pl.BlockSpec((tile, wide), lambda i: (i, 0)),
        out_shape=jax.ShapeDtypeStruct((length, wide), BF16),
        scratch_shapes=[
            pltpu.VMEM((width, wide), BF16),
            pltpu.VMEM((width, wide), BF16),
            pltpu.VMEM((tile + edge, width), BF16),
            pltpu.SemaphoreType.DMA((2 * len(arrays),)),
        ],
        compiler_params=pltpu.CompilerParams(vmem_limit_bytes=50 * 2**20),
        cost_estimate=pl.CostEstimate(
            flops=4 * length * width * wide, bytes_accessed=4 * width * wide, transcendentals=0
        ),
    )(features, halo, taps, *arrays)


def down_kernel(meta, x_ref, *rest):
    *refs, out_ref, down_w, sem = rest
    rows = down_w.shape[0] // lax.axis_size("sp")

    @pl.when(pl.program_id(0) == 0)
    def _():
        copies = load_pieces(meta, refs, ((2 * rows, 3 * rows),), (down_w,), sem)
        finish_pieces(copies)

    wide = out_ref.shape[1]
    part = min(512, wide)
    for col in range(0, wide, part):
        out_ref[:, col : col + part] = mm_nt(x_ref[...], down_w[col : col + part, :]).astype(BF16)


def down_part(hidden, width, pieces):
    length, wide = hidden.shape
    tile = min(512, length)
    meta = [p[:4] for p in pieces]
    arrays = [p[4] for p in pieces]
    return pl.pallas_call(
        functools.partial(down_kernel, meta),
        grid=(length // tile,),
        in_specs=[pl.BlockSpec((tile, wide), lambda i: (i, 0))]
        + [pl.BlockSpec(memory_space=pl.ANY)] * len(arrays),
        out_specs=pl.BlockSpec((tile, width), lambda i: (i, 0)),
        out_shape=jax.ShapeDtypeStruct((length, width), BF16),
        scratch_shapes=[
            pltpu.VMEM((width, wide), BF16),
            pltpu.SemaphoreType.DMA((len(arrays),)),
        ],
        compiler_params=pltpu.CompilerParams(vmem_limit_bytes=50 * 2**20),
        cost_estimate=pl.CostEstimate(
            flops=2 * length * width * wide, bytes_accessed=2 * width * wide, transcendentals=0
        ),
    )(hidden, *arrays)


def finish_kernel(place_ref, all_ref, g_ref, h_ref, gate_ref, coef_ref, out_ref, state_ref):
    @pl.when(pl.program_id(0) == 0)
    def _():
        state_ref[...] = jnp.zeros_like(state_ref)

        def turn(i, carry):
            for unit in range(all_ref.shape[1]):
                block = all_ref[i, unit]
                state_ref[unit] = (
                    mm(block[:, LANES:], state_ref[unit]) + block[:, :LANES].astype(F32)
                )
            return carry

        lax.fori_loop(0, place_ref[0], turn, 0)

    coef = coef_ref[...]
    count = out_ref.shape[1] // LANES // 2
    for head in range(2 * count):
        unit = head if head < count else count + (head - count) // 2
        at = pl.ds(head * LANES, LANES)
        out = mm(g_ref[:, at], state_ref[unit]) + h_ref[:, at]
        gate = gate_ref[:, at].astype(F32)
        scaled = out * lax.rsqrt(jnp.mean(out * out, axis=-1, keepdims=True) + EPSILON) * coef
        out_ref[:, at] = (scaled * (gate / (1.0 + jnp.exp(-gate)))).astype(out_ref.dtype)


def finish_heads(place, everyone, g, h, gates, coef):
    length, wide = g.shape
    tile = min(256, length)
    return pl.pallas_call(
        finish_kernel,
        grid_spec=pltpu.PrefetchScalarGridSpec(
            num_scalar_prefetch=1,
            grid=(length // tile,),
            in_specs=[
                pl.BlockSpec(everyone.shape, lambda i, p: (0, 0, 0, 0)),
                pl.BlockSpec((tile, wide), lambda i, p: (i, 0)),
                pl.BlockSpec((tile, wide), lambda i, p: (i, 0)),
                pl.BlockSpec((tile, wide), lambda i, p: (i, 0)),
                pl.BlockSpec((1, LANES), lambda i, p: (0, 0)),
            ],
            out_specs=pl.BlockSpec((tile, wide), lambda i, p: (i, 0)),
            scratch_shapes=[pltpu.VMEM((everyone.shape[1], LANES, LANES), F32)],
        ),
        out_shape=jax.ShapeDtypeStruct((length, wide), BF16),
        cost_estimate=pl.CostEstimate(
            flops=2 * length * wide * LANES * 8, bytes_accessed=length * wide * 10, transcendentals=0
        ),
    )(place, everyone, g, h, gates, coef)


def per_device(
    arriving_hidden_state,
    former_request_vectors,
    former_match_vectors,
    latter_request_vectors,
    latter_match_vectors,
    stored_vectors_both,
    closing_valve_operands,
    update_level_before_squash,
    fading_data_input,
    sparse_fading_boost,
    unitwise_fading_loglevel,
    fading_constant_term,
    unitwise_normalizer_coef,
    emission_map_weights,
    channel_normalizer_coef,
    switching_channel_map,
    broadening_channel_map,
    timewise_convolve_tapvalues,
    narrowing_map_weights_in,
):
    length = former_request_vectors.shape[0]
    level = (
        -jnp.exp(unitwise_fading_loglevel)[..., None]
        * jax.nn.softplus(fading_data_input + fading_constant_term[..., None])
        + sparse_fading_boost
    )
    beta_rate = jax.nn.sigmoid(update_level_before_squash.astype(jnp.float32))
    gates_beta = jnp.concatenate([level, beta_rate], axis=0).reshape(-1, length)
    gates_beta = jnp.pad(gates_beta, ((0, -gates_beta.shape[0] % 8), (0, 0)))
    spare = -latter_request_vectors.shape[1] % LANES
    sides = jnp.concatenate(
        [switching_channel_map, broadening_channel_map, narrowing_map_weights_in], axis=0
    )
    side = line_step(line_start(sides), 1)
    units = former_request_vectors.shape[1] // LANES + (
        latter_request_vectors.shape[1] + spare
    ) // LANES
    running = jnp.broadcast_to(jnp.eye(LANES, 2 * LANES, LANES, dtype=F32), (units, LANES, 2 * LANES))
    drawn = (
        former_request_vectors,
        former_match_vectors,
        jnp.pad(latter_request_vectors, ((0, 0), (0, spare))),
        jnp.pad(latter_match_vectors, ((0, 0), (0, spare))),
        stored_vectors_both.reshape(length, -1),
        gates_beta,
    )
    parts = 4 if length % (4 * CHUNK) == 0 else 1
    done = ()
    summary = None
    for part in range(parts):
        if part == parts - 1:
            side, running = tie(side, running)
            side = line_step(line_swap(side, 1), 2)
        *done, running, summary = local_terms(*drawn, running, part, parts, tuple(done))
    g_part, h_part = done
    everyone = exchange(summary)
    side, everyone = tie(side, everyone)
    side = line_step(line_swap(side, 2), 3)
    place = lax.axis_index("sp").astype(jnp.int32).reshape(1)
    attended = finish_heads(
        place,
        everyone,
        g_part,
        h_part,
        closing_valve_operands.reshape(length, -1),
        unitwise_normalizer_coef.reshape(1, -1),
    )
    team = lax.axis_size("tp")
    arrived = lax.all_to_all(
        attended.reshape(team, length // team, -1), "tp", split_axis=0, concat_axis=0, tiled=True
    )
    skip_stream, normed = project(
        arrived,
        emission_map_weights,
        arriving_hidden_state,
        channel_normalizer_coef.reshape(1, -1),
    )
    side, normed = tie(side, normed)
    side = line_rest(line_swap(side, 3), 4)
    features = lax.all_gather(normed, "tp", axis=0, tiled=True)
    edge = 16
    halo = from_behind(features[-edge:], "sp", 1)
    taps = timewise_convolve_tapvalues.astype(F32).reshape(2 * TAPS, -1)
    hidden = up_part(features, halo, taps, side["pieces"])
    partial = down_part(hidden, features.shape[1], side["pieces"])
    return (skip_stream + team_sum(partial)).astype(jnp.bfloat16)


def team_sum(partial):
    team = lax.axis_size("tp")
    if team != 4:
        return lax.psum_scatter(partial, "tp", scatter_dimension=0, tiled=True).astype(F32)
    me = lax.axis_index("tp")
    core, place = me % 2, me // 2
    blocks = partial.reshape(2, 2, -1, partial.shape[1])
    away = lax.dynamic_index_in_dim(blocks, 1 - core, 1, False)
    came = lax.ppermute(away, "tp", [(i, i ^ 1) for i in range(team)])
    mine = lax.dynamic_index_in_dim(blocks, core, 1, False)

    def both(which):
        return lax.dynamic_index_in_dim(mine, which, 0, False).astype(F32) + (
            lax.dynamic_index_in_dim(came, which, 0, False).astype(F32)
        )

    across = lax.ppermute(both(1 - place).astype(BF16), "tp", [(i, i ^ 2) for i in range(team)])
    return both(place) + across.astype(F32)


def solution(mesh):
    placed = (
        P(("sp", "tp"), None),
        P("sp", "tp"),
        P("sp", "tp"),
        P("sp", "tp"),
        P("sp", "tp"),
        P("sp", None, "tp"),
        P("sp", None, "tp"),
        P(None, "tp", "sp"),
        P(None, "tp", "sp"),
        P(None, "tp", "sp"),
        P(None, "tp"),
        P(None, "tp"),
        P(),
        P(),
        P(),
        P("sp", "tp"),
        P("sp", "tp"),
        P(None, None, "tp"),
        P("sp", "tp"),
    )
    return jax.shard_map(
        per_device, mesh=mesh, in_specs=placed, out_specs=P(("sp", "tp"), None), check_vma=False
    )
```

```python
import functools

import jax
import jax.numpy as jnp
from jax import lax
from jax.experimental import pallas as pl
from jax.experimental.pallas import tpu as pltpu
from jax.sharding import PartitionSpec as P


TAPS = 3
CHUNK = 128
BASE = 16
LANES = 128

EPSILON = 1e-06
F32 = jnp.float32
BF16 = jnp.bfloat16


def from_behind(value, axis, steps):
    count = lax.axis_size(axis)
    leading, last = (max(0, -steps), min(count, count - steps))
    return lax.ppermute(value, axis, [(source, source + steps) for source in range(leading, last)])


def mm(a, b):
    return jnp.dot(a.astype(BF16), b.astype(BF16), preferred_element_type=F32)


def mm_nt(a, b):
    return lax.dot_general(
        a.astype(BF16), b.astype(BF16), (((1,), (1,)), ((), ())), preferred_element_type=F32
    )


def mm_tn(a, b):
    return mm(a.T, b)


def local_kernel(
    q1_ref, k1_ref, q2_ref, k2_ref, v_ref, gb_ref, from_ref, *rest
):
    g_ref, h_ref, last_ref, sum_ref, run_ref = rest[-5:]
    step = pl.program_id(0)
    count = v_ref.shape[1] // LANES // 2
    pair = 2
    rows = lax.broadcasted_iota(jnp.int32, (CHUNK, CHUNK), 0)
    cols = lax.broadcasted_iota(jnp.int32, (CHUNK, CHUNK), 1)
    eye = (rows == cols).astype(F32)
    causal = rows >= cols
    strict = rows > cols
    lane = lax.broadcasted_iota(jnp.int32, (1, LANES), 1)

    @pl.when(step == 0)
    def _():
        run_ref[...] = from_ref[...]

    gb = gb_ref[...]
    cum = gb
    lanes8 = lax.broadcasted_iota(jnp.int32, gb.shape, 1)
    shift = 1
    while shift < CHUNK:
        cum = cum + jnp.where(lanes8 >= shift, pltpu.roll(cum, shift, 1), 0.0)
        shift *= 2
    gbt = gb.T
    cumt = cum.T

    pend = None
    for head in range(2 * count):
        group, at = head // count, head % count
        if group == 0:
            q = q1_ref[:, at * LANES : (at + 1) * LANES].astype(F32)
            k = k1_ref[:, at * LANES : (at + 1) * LANES].astype(F32)
            key_size = LANES
            own = None
        else:
            key_size = LANES // 2
            own = (lane // key_size) == at % pair
            first = (at // pair) * LANES
            q = jnp.where(own, q2_ref[:, first : first + LANES].astype(F32), 0.0)
            k = jnp.where(own, k2_ref[:, first : first + LANES].astype(F32), 0.0)
        q = q * (lax.rsqrt(jnp.sum(q * q, axis=-1, keepdims=True) + EPSILON) * key_size ** (-0.5))
        k = k * lax.rsqrt(jnp.sum(k * k, axis=-1, keepdims=True) + EPSILON)
        v = v_ref[:, head * LANES : (head + 1) * LANES].astype(F32)
        beta = gbt[:, 2 * count + head : 2 * count + head + 1]
        cum_col = cumt[:, head : head + 1]
        cum_row = cum[head : head + 1, :]
        total = cum[head : head + 1, CHUNK - 1 : CHUNK]
        decay = jnp.exp(jnp.where(causal, cum_col - cum_row, -1e30))
        grown = jnp.exp(cum_col)
        kbeta = k * beta
        kbf = k.astype(BF16)
        low = jnp.where(strict, mm_nt(kbeta, kbf) * decay, 0.0)
        intra = mm_nt(q, kbf) * decay
        base = jnp.where((rows // BASE) == (cols // BASE), low, 0.0)
        power = -base
        inv = eye + power
        size = 2
        while size < BASE:
            power = mm(power, power)
            inv = inv + mm(inv, power)
            size *= 2
        block = BASE
        while block < CHUNK:
            off = jnp.where(
                ((rows // (2 * block)) == (cols // (2 * block)))
                & ((rows // block) != (cols // block)),
                low,
                0.0,
            )
            inv = inv - mm(mm(inv, off), inv)
            block *= 2
        right = jnp.concatenate([v * beta, kbeta * grown], axis=-1)
        solved = mm(inv, right)
        kdec = k * jnp.exp(total - cum_col)
        both = mm_tn(kdec, solved)
        inner = mm(intra, solved)
        unit_diag = eye if own is None else jnp.where(own, eye, 0.0)
        cmap = jnp.exp(total) * unit_diag - both[:, LANES:]
        cadd = both[:, :LANES]
        pmat = q * grown - inner[:, LANES:]
        unit = head if group == 0 else count + at // pair
        run = run_ref[unit]
        seen = mm(pmat, run)
        h_ref[:, head * LANES : (head + 1) * LANES] = seen[:, :LANES] + inner[:, :LANES]
        g_ref[:, head * LANES : (head + 1) * LANES] = seen[:, LANES:].astype(g_ref.dtype)
        if pend is not None:
            cmap = cmap + pend[0]
            cadd = cadd + pend[1]
            pend = None
        if group == 1 and at % pair != pair - 1 and at != count - 1:
            pend = (cmap, cadd)
            continue
        nxt = mm(cmap, run)
        run_ref[unit, :, :LANES] = nxt[:, :LANES] + cadd
        run_ref[unit, :, LANES:] = nxt[:, LANES:]

    @pl.when(step == pl.num_programs(0) - 1)
    def _():
        last_ref[...] = run_ref[...]
        sum_ref[...] = run_ref[...].astype(sum_ref.dtype)


def local_terms(q1, k1, q2, k2, values, gates_beta, running, part, parts, earlier):
    length = q1.shape[0]
    wide = values.shape[1]
    steps = length // CHUNK // parts
    base = part * steps
    units = running.shape[0]
    whole = pl.BlockSpec((units, LANES, 2 * LANES), lambda i: (0, 0, 0))
    return pl.pallas_call(
        local_kernel,
        grid=(steps,),
        in_specs=[
            pl.BlockSpec((CHUNK, q1.shape[1]), lambda i: (i + base, 0)),
            pl.BlockSpec((CHUNK, k1.shape[1]), lambda i: (i + base, 0)),
            pl.BlockSpec((CHUNK, q2.shape[1]), lambda i: (i + base, 0)),
            pl.BlockSpec((CHUNK, k2.shape[1]), lambda i: (i + base, 0)),
            pl.BlockSpec((CHUNK, wide), lambda i: (i + base, 0)),
            pl.BlockSpec((gates_beta.shape[0], CHUNK), lambda i: (0, i + base)),
            whole,
        ]
        + [pl.BlockSpec(memory_space=pl.ANY)] * len(earlier),
        out_specs=[
            pl.BlockSpec((CHUNK, wide), lambda i: (i + base, 0)),
            pl.BlockSpec((CHUNK, wide), lambda i: (i + base, 0)),
            whole,
            whole,
        ],
        out_shape=[
            jax.ShapeDtypeStruct((length, wide), BF16),
            jax.ShapeDtypeStruct((length, wide), F32),
            jax.ShapeDtypeStruct((units, LANES, 2 * LANES), F32),
            jax.ShapeDtypeStruct((units, LANES, 2 * LANES), BF16),
        ],
        scratch_shapes=[pltpu.VMEM((units, LANES, 2 * LANES), F32)],
        input_output_aliases={7 + i: i for i in range(len(earlier))},
        cost_estimate=pl.CostEstimate(
            flops=steps * 4 * 400 * CHUNK**3, bytes_accessed=length * wide * 10, transcendentals=0
        ),
    )(q1, k1, q2, k2, values, gates_beta, running, *earlier)


def exchange_kernel(own_ref, all_ref, send_sem, recv_sem):
    me = lax.axis_index("sp")
    count = all_ref.shape[0]
    barrier = pltpu.get_barrier_semaphore()
    for gap in range(1, count):
        pl.semaphore_signal(
            barrier,
            inc=1,
            device_id={"sp": lax.rem(me + gap, count)},
            device_id_type=pl.DeviceIdType.MESH,
        )
    pl.semaphore_wait(barrier, count - 1)

    def copy(source, target):
        return pltpu.make_async_remote_copy(
            src_ref=own_ref,
            dst_ref=all_ref.at[source],
            send_sem=send_sem.at[target],
            recv_sem=recv_sem.at[source],
            device_id={"sp": target},
            device_id_type=pl.DeviceIdType.MESH,
        )

    for target in range(1, count):
        @pl.when(me < target)
        def _():
            copy(me, target).start()

    for source in range(count - 1):
        @pl.when(source < me)
        def _():
            copy(source, me).wait_recv()

    for target in range(1, count):
        @pl.when(me < target)
        def _():
            copy(me, target).wait_send()


def exchange(summary):
    count = lax.axis_size("sp")
    return pl.pallas_call(
        exchange_kernel,
        in_specs=[pl.BlockSpec(memory_space=pltpu.VMEM)],
        out_specs=pl.BlockSpec(memory_space=pltpu.VMEM),
        out_shape=jax.ShapeDtypeStruct((count, *summary.shape), summary.dtype),
        scratch_shapes=[pltpu.SemaphoreType.DMA((count,)), pltpu.SemaphoreType.DMA((count,))],
        compiler_params=pltpu.CompilerParams(collective_id=1, has_side_effects=True),
        cost_estimate=pl.CostEstimate(flops=10**9, bytes_accessed=10**6, transcendentals=0),
    )(summary)


def swapped(value, low, high):
    places = [2 * place + parity for place in range(low, high) for parity in range(2)]
    return lax.ppermute(value, "sp", [(i, i ^ 1) for i in places])


def line_start(own):
    ring = lax.axis_size("sp") // 2
    return dict(
        right=own, left=own, pieces=[(0, 0, 0, ring, own), (0, 1, 0, ring, swapped(own, 0, ring))]
    )


def line_step(line, gap):
    ring = lax.axis_size("sp") // 2
    if gap >= ring:
        return line
    up = [(2 * p + q, 2 * p + 2 + q) for p in range(gap - 1, ring - 1) for q in range(2)]
    down = [(2 * p + q, 2 * p - 2 + q) for p in range(1, ring - gap + 1) for q in range(2)]
    right = lax.ppermute(line["right"], "sp", up)
    left = lax.ppermute(line["left"], "sp", down)
    pieces = [(gap, 0, gap, ring, right), (ring - gap, 0, 0, ring - gap, left)]
    return dict(right=right, left=left, pieces=line["pieces"] + pieces)


def line_swap(line, gap):
    ring = lax.axis_size("sp") // 2
    if gap >= ring:
        return line
    pieces = [
        (gap, 1, gap, ring, swapped(line["right"], gap, ring)),
        (ring - gap, 1, 0, ring - gap, swapped(line["left"], 0, ring - gap)),
    ]
    return dict(line, pieces=line["pieces"] + pieces)


def line_rest(line, gap):
    ring = lax.axis_size("sp") // 2
    for more in range(gap, ring):
        line = line_swap(line_step(line, more), more)
    return line


def tie(line, other):
    other, right, left = lax.optimization_barrier((other, line["right"], line["left"]))
    return dict(line, right=right, left=left), other


def load_pieces(meta, refs, ranges, targets, sem):
    me = lax.axis_index("sp")
    ring = lax.axis_size("sp") // 2
    place = me // 2
    copies = []
    for (gap, other, low_place, high_place), ref in zip(meta, refs):
        owner = lax.rem(place + ring - gap, ring) * 2 + (lax.rem(me, 2) + other) % 2
        valid = (place >= low_place) & (place < high_place)
        for index, (low, high) in enumerate(ranges):
            size = high - low
            one = pltpu.make_async_copy(
                ref.at[pl.ds(low, size), :],
                targets[index].at[pl.ds(pl.multiple_of(owner * size, 16), size), :],
                sem.at[len(copies)],
            )
            copies.append((valid, one))

    for valid, one in copies:
        @pl.when(valid)
        def _():
            one.start()

    return copies


def finish_pieces(copies):
    for valid, one in copies:
        @pl.when(valid)
        def _():
            one.wait()


def project_kernel(x_ref, w_ref, skip_ref, coef_ref, sum_ref, out_ref):
    step = pl.program_id(0)

    @pl.when(step == 0)
    def _():
        sum_ref[...] = skip_ref[...].astype(F32)

    sum_ref[...] += jnp.dot(x_ref[0], w_ref[...], preferred_element_type=F32)

    @pl.when(step == pl.num_programs(0) - 1)
    def _():
        total = sum_ref[...]
        scale = lax.rsqrt(jnp.mean(total * total, axis=-1, keepdims=True) + EPSILON)
        out_ref[...] = (total * scale * coef_ref[...]).astype(out_ref.dtype)


def project(x, weights, skip, coef):
    team, rows, wide = x.shape
    depth, width = weights.shape
    part = wide // 2
    whole = pl.BlockSpec((rows, width), lambda i: (0, 0))
    return pl.pallas_call(
        project_kernel,
        grid=(depth // part,),
        in_specs=[
            pl.BlockSpec((1, rows, part), lambda i: (i // 2, 0, i % 2)),
            pl.BlockSpec((part, width), lambda i: ((i % 2) * team + i // 2, 0)),
            whole,
            pl.BlockSpec((1, width), lambda i: (0, 0)),
        ],
        out_specs=[whole, whole],
        out_shape=[
            jax.ShapeDtypeStruct((rows, width), F32),
            jax.ShapeDtypeStruct((rows, width), BF16),
        ],
        cost_estimate=pl.CostEstimate(
            flops=2 * rows * depth * width, bytes_accessed=2 * depth * width, transcendentals=0
        ),
    )(x, weights, skip, coef)


def up_kernel(meta, x_ref, halo_ref, taps_ref, *rest):
    *refs, out_ref, gate_w, up_w, xs, sem = rest
    tile = x_ref.shape[0]
    step = pl.program_id(0)
    edge = halo_ref.shape[0]
    rows = gate_w.shape[0] // lax.axis_size("sp")

    @pl.when(step == 0)
    def _():
        copies = load_pieces(meta, refs, ((0, rows), (rows, 2 * rows)), (gate_w, up_w), sem)
        xs[:edge, :] = halo_ref[...]
        finish_pieces(copies)

    @pl.when(step > 0)
    def _():
        xs[:edge, :] = xs[tile:, :]

    xs[edge:, :] = x_ref[...]
    wide = out_ref.shape[1]
    part = min(256, wide)
    for col in range(0, wide, part):
        at = slice(col, col + part)
        taken = []
        for which, w in enumerate((gate_w, up_w)):
            low = jnp.dot(xs[...], w[:, at], preferred_element_type=F32)
            low = low.astype(BF16).astype(F32)
            total = 0.0
            for tap in range(TAPS):
                moved = low[edge - TAPS + 1 + tap : edge - TAPS + 1 + tap + tile]
                total = total + taps_ref[2 * tap + which : 2 * tap + which + 1, at] * moved
            taken.append(total)
        gate, up = taken
        out_ref[:, at] = (gate / (1.0 + jnp.exp(-gate)) * up).astype(out_ref.dtype)


def up_part(features, halo, taps, pieces):
    length, width = features.shape
    wide = taps.shape[1]
    tile = min(512, length)
    meta = [p[:4] for p in pieces]
    arrays = [p[4] for p in pieces]
    edge = halo.shape[0]
    return pl.pallas_call(
        functools.partial(up_kernel, meta),
        grid=(length // tile,),
        in_specs=[
            pl.BlockSpec((tile, width), lambda i: (i, 0)),
            pl.BlockSpec(halo.shape, lambda i: (0, 0)),
            pl.BlockSpec(taps.shape, lambda i: (0, 0)),
        ]
        + [pl.BlockSpec(memory_space=pl.ANY)] * len(arrays),
        out_specs=pl.BlockSpec((tile, wide), lambda i: (i, 0)),
        out_shape=jax.ShapeDtypeStruct((length, wide), BF16),
        scratch_shapes=[
            pltpu.VMEM((width, wide), BF16),
            pltpu.VMEM((width, wide), BF16),
            pltpu.VMEM((tile + edge, width), BF16),
            pltpu.SemaphoreType.DMA((2 * len(arrays),)),
        ],
        compiler_params=pltpu.CompilerParams(vmem_limit_bytes=50 * 2**20),
        cost_estimate=pl.CostEstimate(
            flops=4 * length * width * wide, bytes_accessed=4 * width * wide, transcendentals=0
        ),
    )(features, halo, taps, *arrays)


def down_kernel(meta, x_ref, *rest):
    *refs, out_ref, down_w, sem = rest
    rows = down_w.shape[0] // lax.axis_size("sp")

    @pl.when(pl.program_id(0) == 0)
    def _():
        copies = load_pieces(meta, refs, ((0, rows),), (down_w,), sem)
        finish_pieces(copies)

    wide = out_ref.shape[1]
    part = min(512, wide)
    for col in range(0, wide, part):
        out_ref[:, col : col + part] = mm_nt(x_ref[...], down_w[col : col + part, :]).astype(BF16)


def down_part(hidden, width, pieces):
    length, wide = hidden.shape
    tile = min(512, length)
    meta = [p[:4] for p in pieces]
    arrays = [p[4] for p in pieces]
    return pl.pallas_call(
        functools.partial(down_kernel, meta),
        grid=(length // tile,),
        in_specs=[pl.BlockSpec((tile, wide), lambda i: (i, 0))]
        + [pl.BlockSpec(memory_space=pl.ANY)] * len(arrays),
        out_specs=pl.BlockSpec((tile, width), lambda i: (i, 0)),
        out_shape=jax.ShapeDtypeStruct((length, width), BF16),
        scratch_shapes=[
            pltpu.VMEM((width, wide), BF16),
            pltpu.SemaphoreType.DMA((len(arrays),)),
        ],
        compiler_params=pltpu.CompilerParams(vmem_limit_bytes=50 * 2**20),
        cost_estimate=pl.CostEstimate(
            flops=2 * length * width * wide, bytes_accessed=2 * width * wide, transcendentals=0
        ),
    )(hidden, *arrays)


def finish_kernel(place_ref, all_ref, g_ref, h_ref, gate_ref, coef_ref, out_ref, state_ref):
    @pl.when(pl.program_id(0) == 0)
    def _():
        state_ref[...] = jnp.zeros_like(state_ref)

        def turn(i, carry):
            for unit in range(all_ref.shape[1]):
                block = all_ref[i, unit]
                state_ref[unit] = (
                    mm(block[:, LANES:], state_ref[unit]) + block[:, :LANES].astype(F32)
                )
            return carry

        lax.fori_loop(0, place_ref[0], turn, 0)

    coef = coef_ref[...]
    count = out_ref.shape[1] // LANES // 2
    for head in range(2 * count):
        unit = head if head < count else count + (head - count) // 2
        at = pl.ds(head * LANES, LANES)
        out = mm(g_ref[:, at], state_ref[unit]) + h_ref[:, at]
        gate = gate_ref[:, at].astype(F32)
        scaled = out * lax.rsqrt(jnp.mean(out * out, axis=-1, keepdims=True) + EPSILON) * coef
        out_ref[:, at] = (scaled * (gate / (1.0 + jnp.exp(-gate)))).astype(out_ref.dtype)


def finish_heads(place, everyone, g, h, gates, coef):
    length, wide = g.shape
    tile = min(256, length)
    return pl.pallas_call(
        finish_kernel,
        grid_spec=pltpu.PrefetchScalarGridSpec(
            num_scalar_prefetch=1,
            grid=(length // tile,),
            in_specs=[
                pl.BlockSpec(everyone.shape, lambda i, p: (0, 0, 0, 0)),
                pl.BlockSpec((tile, wide), lambda i, p: (i, 0)),
                pl.BlockSpec((tile, wide), lambda i, p: (i, 0)),
                pl.BlockSpec((tile, wide), lambda i, p: (i, 0)),
                pl.BlockSpec((1, LANES), lambda i, p: (0, 0)),
            ],
            out_specs=pl.BlockSpec((tile, wide), lambda i, p: (i, 0)),
            scratch_shapes=[pltpu.VMEM((everyone.shape[1], LANES, LANES), F32)],
        ),
        out_shape=jax.ShapeDtypeStruct((length, wide), BF16),
        cost_estimate=pl.CostEstimate(
            flops=2 * length * wide * LANES * 8, bytes_accessed=length * wide * 10, transcendentals=0
        ),
    )(place, everyone, g, h, gates, coef)


def per_device(
    arriving_hidden_state,
    former_request_vectors,
    former_match_vectors,
    latter_request_vectors,
    latter_match_vectors,
    stored_vectors_both,
    closing_valve_operands,
    update_level_before_squash,
    fading_data_input,
    sparse_fading_boost,
    unitwise_fading_loglevel,
    fading_constant_term,
    unitwise_normalizer_coef,
    emission_map_weights,
    channel_normalizer_coef,
    switching_channel_map,
    broadening_channel_map,
    timewise_convolve_tapvalues,
    narrowing_map_weights_in,
):
    length = former_request_vectors.shape[0]
    level = (
        -jnp.exp(unitwise_fading_loglevel)[..., None]
        * jax.nn.softplus(fading_data_input + fading_constant_term[..., None])
        + sparse_fading_boost
    )
    beta_rate = jax.nn.sigmoid(update_level_before_squash.astype(jnp.float32))
    gates_beta = jnp.concatenate([level, beta_rate], axis=0).reshape(-1, length)
    gates_beta = jnp.pad(gates_beta, ((0, -gates_beta.shape[0] % 8), (0, 0)))
    spare = -latter_request_vectors.shape[1] % LANES
    sides = jnp.concatenate([switching_channel_map, broadening_channel_map], axis=0)
    side = line_step(line_start(sides), 1)
    units = former_request_vectors.shape[1] // LANES + (
        latter_request_vectors.shape[1] + spare
    ) // LANES
    running = jnp.broadcast_to(jnp.eye(LANES, 2 * LANES, LANES, dtype=F32), (units, LANES, 2 * LANES))
    drawn = (
        former_request_vectors,
        former_match_vectors,
        jnp.pad(latter_request_vectors, ((0, 0), (0, spare))),
        jnp.pad(latter_match_vectors, ((0, 0), (0, spare))),
        stored_vectors_both.reshape(length, -1),
        gates_beta,
    )
    parts = 4 if length % (4 * CHUNK) == 0 else 1
    done = ()
    summary = None
    for part in range(parts):
        if part == parts // 2:
            side, running = tie(side, running)
            side = line_step(line_swap(side, 1), 2)
        *done, running, summary = local_terms(*drawn, running, part, parts, tuple(done))
    g_part, h_part = done
    everyone = exchange(summary)
    side, (everyone, narrow) = tie(side, (everyone, narrowing_map_weights_in))
    side = line_step(line_swap(side, 2), 3)
    down = line_step(line_start(narrow), 1)
    place = lax.axis_index("sp").astype(jnp.int32).reshape(1)
    attended = finish_heads(
        place,
        everyone,
        g_part,
        h_part,
        closing_valve_operands.reshape(length, -1),
        unitwise_normalizer_coef.reshape(1, -1),
    )
    team = lax.axis_size("tp")
    arrived = lax.all_to_all(
        attended.reshape(team, length // team, -1), "tp", split_axis=0, concat_axis=0, tiled=True
    )
    skip_stream, normed = project(
        arrived,
        emission_map_weights,
        arriving_hidden_state,
        channel_normalizer_coef.reshape(1, -1),
    )
    side, normed = tie(side, normed)
    side = line_rest(line_swap(side, 3), 4)
    features = lax.all_gather(normed, "tp", axis=0, tiled=True)
    down = line_step(line_swap(down, 1), 2)
    edge = 16
    halo = from_behind(features[-edge:], "sp", 1)
    taps = timewise_convolve_tapvalues.astype(F32).reshape(2 * TAPS, -1)
    down, halo = tie(down, halo)
    down = line_step(line_swap(down, 2), 3)
    hidden = up_part(features, halo, taps, side["pieces"])
    down = line_rest(line_swap(down, 3), 4)
    partial = down_part(hidden, features.shape[1], down["pieces"])
    return (skip_stream + team_sum(partial)).astype(jnp.bfloat16)


def team_sum(partial):
    team = lax.axis_size("tp")
    if team != 4:
        return lax.psum_scatter(partial, "tp", scatter_dimension=0, tiled=True).astype(F32)
    me = lax.axis_index("tp")
    core, place = me % 2, me // 2
    blocks = partial.reshape(2, 2, -1, partial.shape[1])
    away = lax.dynamic_index_in_dim(blocks, 1 - core, 1, False)
    came = lax.ppermute(away, "tp", [(i, i ^ 1) for i in range(team)])
    mine = lax.dynamic_index_in_dim(blocks, core, 1, False)

    def both(which):
        return lax.dynamic_index_in_dim(mine, which, 0, False).astype(F32) + (
            lax.dynamic_index_in_dim(came, which, 0, False).astype(F32)
        )

    across = lax.ppermute(both(1 - place).astype(BF16), "tp", [(i, i ^ 2) for i in range(team)])
    return both(place) + across.astype(F32)


def solution(mesh):
    placed = (
        P(("sp", "tp"), None),
        P("sp", "tp"),
        P("sp", "tp"),
        P("sp", "tp"),
        P("sp", "tp"),
        P("sp", None, "tp"),
        P("sp", None, "tp"),
        P(None, "tp", "sp"),
        P(None, "tp", "sp"),
        P(None, "tp", "sp"),
        P(None, "tp"),
        P(None, "tp"),
        P(),
        P(),
        P(),
        P("sp", "tp"),
        P("sp", "tp"),
        P(None, None, "tp"),
        P("sp", "tp"),
    )
    return jax.shard_map(
        per_device, mesh=mesh, in_specs=placed, out_specs=P(("sp", "tp"), None), check_vma=False
    )
```
